32 devices in a mesh: tp: 8 (over z, y), dp: 4 (over x, core).
Axes of the slice: x: 2, y: 2, z: 4, core: 2. Of those that a mesh axis runs over, the one named last changes fastest.
Arguments:
- tokens: bfloat16 [128, 4096], P('tp', 'dp'), may hold values from -10 to 10
- norm_gain: float32 [2, 4096], P(None, 'dp'), may hold values from 0.1 to 1.9
- input_weight: bfloat16 [2, 4096, 1024], P(None, 'dp', 'tp'), may hold values from -0.09375 to 0.09375
- decay_rate: float32 [2, 64, 64], P(None, 'tp'), may hold values from 0.01 to 1
- frequency: float32 [2, 64, 64], P(None, 'tp'), may hold values from 0.5 to 3
- step_size: float32 [2, 64], P(None, 'tp'), may hold values from 0.1 to 1
- state_in: float32 [2, 64, 16, 128], P(None, 'tp'), may hold values from -1.5 to 1.5
- readout: float32 [2, 64, 16, 128], P(None, 'tp'), may hold values from -0.5 to 0.5
- skip_gain: float32 [2, 1024], P(None, 'tp'), may hold values from -3 to 3
- value_weight: bfloat16 [2, 1024, 4096], P(None, 'tp', 'dp'), may hold values from -0.1875 to 0.1875
- gate_weight: bfloat16 [2, 1024, 4096], P(None, 'tp', 'dp'), may hold values from -0.1875 to 0.1875
- states: float32 [2, 128, 64, 128], P(None, 'dp', 'tp'), may hold values from -3 to 3
Outputs:
- tokens_out: bfloat16 [128, 4096], P('tp', 'dp')
- states_out: float32 [2, 128, 64, 128], P(None, 'dp', 'tp')
The draws below stay inside these ranges and needn't reach their ends.
All inputs are finite; a program needn't handle non-finite values.
Results may differ from the reference program's by a relative error of at most 0.007.
Values may be sent and summed in bfloat16 or wider, within the bound.
A program may use at most 64 MiB of HBM per device.

```python
import math
import jax
import jax.numpy as jnp
from jax import lax

D = 4096
S = 1024
GS = 16
P_SIZE = 64
LAYERS = 2
G = 64
BATCH = 128


def draw_tokens(key, part):
    first, second, third = jax.random.split(key, 3)
    column_scale = jnp.exp(jax.random.uniform(second, (32,), jnp.float32, -0.7, 0.7))
    column_scale = jnp.repeat(column_scale, D // 32)
    base = jnp.clip(jax.random.normal(first, (BATCH, D), jnp.float32), -4.0, 4.0)
    return (base * column_scale[None, :]).astype(jnp.bfloat16)


def steps_of(stream_key, dims, pieces, smallest, top_value):
    def one(position, blocks):
        steps = jax.random.uniform(jax.random.fold_in(jax.random.fold_in(stream_key, 6), position), (blocks,), jnp.float32, smallest / len(pieces), top_value / len(pieces))
        return jnp.repeat(jnp.exp(steps), dims[position] // blocks).reshape((-1,) + (1,) * (len(dims) - position - 1))

    level = one(*pieces[0])
    for cut in pieces[1:]:
        level = level * one(*cut)
    return level


def bell_draw(stream_key, dims, spread, most, pieces=(), dtype=jnp.bfloat16):
    result = jax.random.normal(stream_key, dims, jnp.float32) * spread
    if len(pieces) > 0:
        result = steps_of(stream_key, dims, pieces, -0.22, 0.18) * result
    return jnp.clip(result, min=-most, max=most).astype(dtype)


def setup_inputs(seed: int = 0) -> dict:
    seeds = jax.random.split(jax.random.key(seed), 13)
    tokens = draw_tokens(jax.random.fold_in(seeds[12], 71), 0)
    norm_gain = jnp.clip(1.0 + 0.18 * jax.random.normal(seeds[1], (LAYERS, D), jnp.float32), 0.1, 1.9)
    input_weight = bell_draw(seeds[2], (LAYERS, D, S), D ** -0.5, 0.09375, ((1, 4), (2, 8)))
    decay_rate = jnp.clip(jnp.exp(math.log(1.0) - 4.6051702 * jax.random.uniform(seeds[3], (LAYERS, G, P_SIZE), jnp.float32) ** steps_of(seeds[3], (LAYERS, G, P_SIZE), ((1, 8),), -0.2, 0.2)), 0.01, 1.0)
    frequency = jnp.clip(0.5 + 2.5 * jax.random.uniform(seeds[4], (LAYERS, G, P_SIZE), jnp.float32) ** steps_of(seeds[4], (LAYERS, G, P_SIZE), ((1, 8),), -0.2, 0.2), 0.5, 3.0)
    step_size = jnp.clip(jnp.exp(math.log(1.0) - 2.3025851 * jax.random.uniform(seeds[5], (LAYERS, G), jnp.float32) ** steps_of(seeds[5], (LAYERS, G), ((1, 8),), -0.2, 0.2)), 0.1, 1.0)
    state_in = bell_draw(seeds[6], (LAYERS, G, GS, 2 * P_SIZE), GS ** -0.5, 1.5, ((1, 8),), jnp.float32)
    readout = bell_draw(seeds[7], (LAYERS, G, GS, 2 * P_SIZE), (2 * P_SIZE) ** -0.5, 0.5, ((1, 8),), jnp.float32)
    skip_gain = bell_draw(seeds[8], (LAYERS, S), 0.5, 3.0, ((1, 8),), jnp.float32)
    value_weight = bell_draw(seeds[9], (LAYERS, S, D), S ** -0.5, 0.1875, ((1, 8), (2, 4)))
    gate_weight = bell_draw(seeds[10], (LAYERS, S, D), S ** -0.5, 0.1875, ((1, 8), (2, 4)))
    states = bell_draw(seeds[11], (LAYERS, BATCH, G, 2 * P_SIZE), 0.5, 3.0, ((1, 4), (2, 8)), jnp.float32)
    return dict(tokens=tokens, norm_gain=norm_gain, input_weight=input_weight, decay_rate=decay_rate, frequency=frequency, step_size=step_size, state_in=state_in, readout=readout, skip_gain=skip_gain, value_weight=value_weight, gate_weight=gate_weight, states=states)


epsilon = 1e-06

def transition(rate, frequency, step):
    magnitude = jnp.exp(-rate * step[:, None])
    angle = frequency * step[:, None]
    keep_real = magnitude * jnp.cos(angle)
    keep_imag = magnitude * jnp.sin(angle)
    minus_one = keep_real - 1.0
    denominator = rate * rate + frequency * frequency
    lift_real = (-minus_one * rate + keep_imag * frequency) / denominator
    lift_imag = (-keep_imag * rate - minus_one * frequency) / denominator
    return (keep_real, keep_imag, lift_real, lift_imag)

def update(drive, state, rate, frequency, step, state_in, readout, skip):
    groups = rate.shape[0]
    half = state.shape[-1] // 2
    grouped = drive.reshape(drive.shape[0], groups, -1)
    pushed = jnp.einsum('sgc,gcq->sgq', grouped, state_in, precision=lax.Precision.HIGHEST)
    keep_real, keep_imag, lift_real, lift_imag = transition(rate, frequency, step)
    push_real, push_imag = (pushed[..., :half], pushed[..., half:])
    old_real, old_imag = (state[..., :half], state[..., half:])
    new_real = keep_real * old_real - keep_imag * old_imag + lift_real * push_real - lift_imag * push_imag
    new_imag = keep_real * old_imag + keep_imag * old_real + lift_real * push_imag + lift_imag * push_real
    new_state = jnp.concatenate([new_real, new_imag], axis=-1)
    summed = jnp.einsum('sgq,gcq->sgc', new_state, readout, precision=lax.Precision.HIGHEST)
    value = summed.reshape(drive.shape) + skip[None, :] * drive
    return (new_state, jax.nn.gelu(value).astype(jnp.bfloat16))

def reference(tokens, norm_gain, input_weight, decay_rate, frequency, step_size, state_in, readout, skip_gain, value_weight, gate_weight, states):
    current = tokens
    updated = []
    for depth_index in range(LAYERS):
        widened = current.astype(jnp.float32)
        mean_square = lax.optimization_barrier(jnp.mean(widened * widened, axis=1))
        gained = (widened * norm_gain[depth_index][None, :]).astype(jnp.bfloat16)
        drive = jnp.dot(gained, input_weight[depth_index], preferred_element_type=jnp.float32)
        drive = drive * lax.rsqrt(mean_square + epsilon)[:, None]
        new_state, readout_value = update(drive, states[depth_index], decay_rate[depth_index], frequency[depth_index], step_size[depth_index], state_in[depth_index], readout[depth_index], skip_gain[depth_index])
        updated.append(new_state)
        value = jnp.dot(readout_value, value_weight[depth_index], preferred_element_type=jnp.float32)
        gate = jnp.dot(readout_value, gate_weight[depth_index], preferred_element_type=jnp.float32)
        current = (widened + value * jax.nn.sigmoid(gate)).astype(jnp.bfloat16)
    return (current, jnp.stack(updated))
```

```python
import functools

import jax
import jax.numpy as jnp
from jax import lax
from jax.experimental import pallas as pl
from jax.experimental.pallas import tpu as pltpu
from jax.sharding import PartitionSpec as P

epsilon = 1e-06
HIGHEST = lax.Precision.HIGHEST
NT = (((1,), (1,)), ((), ()))


def iota(shape, axis):
    return lax.broadcasted_iota(jnp.int32, shape, axis)


def kernel(n_tp, n_dp, width, *refs):
    ins, refs = refs[:12], refs[12:]
    (out_tok, out_st), refs = refs[:2], refs[2:]
    held, refs = refs[:11], refs[11:]
    (gain_v, win_v, rate_v, freq_v, step_v, sin_v, rout_v, skip_v, vw_v, gw_v, st_v) = held
    (xg, sq_s, sq_r, part_s, part_r, ready, prod_s, prod_r, keep_v, base_v, lift_v, mix_v, new_v,
     load_sem, out_sem, x_sem, sq_sem, part_sem, ready_sem, prod_sem) = refs
    layers, rows, groups, entries = st_v.shape
    chans = part_s.shape[-1]
    per = chans // groups
    batch = n_dp * rows
    local = xg.shape[-1]
    t = lax.axis_index("tp")
    d = lax.axis_index("dp")

    loads = [pltpu.make_async_copy(ins[0], xg.at[0, t], load_sem.at[0])]
    for i in range(11):
        loads.append(pltpu.make_async_copy(ins[i + 1], held[i], load_sem.at[i + 1]))
    for i in (0, 3, 4, 5, 6, 7, 11, 8, 1, 2, 9, 10):
        loads[i].start()

    barrier = pltpu.get_barrier_semaphore()
    for k in range(1, n_tp):
        pl.semaphore_signal(barrier, inc=1, device_id={"tp": lax.rem(t + k, n_tp)},
                            device_id_type=pl.DeviceIdType.MESH)
    for k in range(1, n_dp):
        pl.semaphore_signal(barrier, inc=1, device_id={"dp": lax.rem(d + k, n_dp)},
                            device_id_type=pl.DeviceIdType.MESH)

    pending = []

    def send(axis, k, src, dst, sems, index):
        me, n = (t, n_tp) if axis == "tp" else (d, n_dp)
        copy = pltpu.make_async_remote_copy(
            src_ref=src, dst_ref=dst,
            send_sem=sems.at[(0,) + index], recv_sem=sems.at[(1,) + index],
            device_id={axis: lax.rem(me + k, n)}, device_id_type=pl.DeviceIdType.MESH)
        copy.start()
        pending.append(copy)
        return copy

    def send_tokens(layer):
        return [send("tp", k, xg.at[layer, t], xg.at[layer, t], x_sem, (layer, k))
                for k in range(1, n_tp)]

    def prepare(layer):
        half = entries // 2
        diagonal = iota((groups, groups), 0) == iota((groups, groups), 1)
        step = jnp.sum(jnp.where(diagonal, step_v[layer][None, :], 0.0), axis=1, keepdims=True)
        rate = jnp.concatenate([rate_v[layer]] * 2, axis=1)
        freq = jnp.concatenate([freq_v[layer]] * 2, axis=1)
        sign = jnp.where(iota((groups, entries), 1) < half, -1.0, 1.0)
        magnitude = jnp.exp(-rate * step)
        angle = freq * step
        keep_real = magnitude * jnp.cos(angle)
        keep_imag = magnitude * jnp.sin(angle)
        minus_one = keep_real - 1.0
        denominator = rate * rate + freq * freq
        lift_real = (-minus_one * rate + keep_imag * freq) / denominator
        lift_imag = sign * (-keep_imag * rate - minus_one * freq) / denominator
        keep_imag = sign * keep_imag

        def swap(value):
            return jnp.concatenate([value[..., half:], value[..., :half]], axis=-1)

        matrix = sin_v[layer]
        lifted = lift_real[:, None, :] * matrix + lift_imag[:, None, :] * swap(matrix)
        lifted = lifted.reshape(chans, entries)
        read = rout_v[layer].reshape(chans, entries)
        mixed = lax.dot_general(lifted, read, NT, precision=HIGHEST,
                                preferred_element_type=jnp.float32)
        first, second = iota((chans, chans), 0), iota((chans, chans), 1)
        mixed = jnp.where(first // per == second // per, mixed, 0.0)
        mixed = mixed + jnp.where(first == second, skip_v[layer][None, :], 0.0)
        old = st_v[layer]
        kept = keep_real[None] * old + keep_imag[None] * swap(old)
        base = lax.dot_general(kept.reshape(rows * groups, entries), read, NT, precision=HIGHEST,
                               preferred_element_type=jnp.float32).reshape(rows, groups, chans)
        own = iota((groups, chans), 0) == iota((groups, chans), 1) // per
        keep_v[layer] = kept
        base_v[layer] = jnp.sum(jnp.where(own[None], base, 0.0), axis=1)
        lift_v[layer] = lifted
        mix_v[layer] = mixed

    loads[0].wait()
    pl.semaphore_wait(barrier, n_tp + n_dp - 2)
    sent = send_tokens(0)
    for i in (3, 4, 5, 6, 7, 11, 8):
        loads[i].wait()
    prepare(0)
    for i in (1, 2, 9, 10):
        loads[i].wait()
    outs = []

    for layer in range(layers):
        for copy in sent:
            copy.wait_recv()
        x = xg[layer].reshape(batch, local).astype(jnp.float32)
        square = jnp.sum(x * x, axis=1, keepdims=True)
        eye = iota((batch, batch), 0) == iota((batch, batch), 1)
        line = jnp.sum(jnp.where(eye, square, 0.0), axis=0, keepdims=True)
        sq_s[layer] = jnp.broadcast_to(line, (8, batch))
        sent = [send("dp", k, sq_s.at[layer], sq_r.at[layer, d], sq_sem, (layer, k))
                for k in range(1, n_dp)]
        gained = (x * gain_v[layer][None, :]).astype(jnp.bfloat16)
        part = jnp.dot(gained, win_v[layer], preferred_element_type=jnp.float32)
        part_s[layer] = part.reshape(n_dp, rows, chans)
        for k in range(1, n_dp):
            sent.append(send("dp", k, part_s.at[layer, lax.rem(d + k, n_dp)],
                             part_r.at[layer, d], part_sem, (layer, k)))
        total = part_s[layer, d]
        for copy in sent:
            copy.wait_recv()
        for k in range(1, n_dp):
            source = lax.rem(d + n_dp - k, n_dp)
            total += part_r[layer, source]
            line += sq_r[layer, source][:1]
        pick = iota((rows, batch), 1) == iota((rows, batch), 0) + d * rows
        square = jnp.sum(jnp.where(pick, line, 0.0), axis=1, keepdims=True)
        drive = total * lax.rsqrt(square / width + epsilon)
        value = base_v[layer] + jnp.dot(drive, mix_v[layer], precision=HIGHEST,
                                        preferred_element_type=jnp.float32)
        ready[layer, d] = jax.nn.gelu(value).astype(jnp.bfloat16)
        sent = [send("dp", k, ready.at[layer, d], ready.at[layer, d], ready_sem, (layer, k))
                for k in range(1, n_dp)]
        own = iota((groups, chans), 0) == iota((groups, chans), 1) // per
        spread = jnp.where(own[None], drive[:, None, :], 0.0).reshape(rows * groups, chans)
        push = jnp.dot(spread, lift_v[layer], precision=HIGHEST, preferred_element_type=jnp.float32)
        new_v[layer] = keep_v[layer] + push.reshape(rows, groups, entries)
        out = pltpu.make_async_copy(new_v.at[layer], out_st.at[layer], out_sem.at[layer])
        out.start()
        outs.append(out)
        for copy in sent:
            copy.wait_recv()
        every = ready[layer].reshape(batch, chans)
        for half, weight in ((0, vw_v), (1, gw_v)):
            product = jnp.dot(every, weight[layer], preferred_element_type=jnp.float32)
            prod_s[layer, half] = product.astype(jnp.bfloat16).reshape(n_tp, batch // n_tp, local)
        sent = []
        for half in range(2):
            for k in range(1, n_tp):
                sent.append(send("tp", k, prod_s.at[layer, half, lax.rem(t + k, n_tp)],
                                 prod_r.at[layer, half, t], prod_sem, (layer, half, k)))
        if layer + 1 < layers:
            prepare(layer + 1)
        for copy in sent:
            copy.wait_recv()
        both = []
        for half in range(2):
            total = prod_s[layer, half, t].astype(jnp.float32)
            for k in range(1, n_tp):
                total += prod_r[layer, half, lax.rem(t + n_tp - k, n_tp)].astype(jnp.float32)
            both.append(total)
        current = xg[layer, t].astype(jnp.float32) + both[0] * jax.nn.sigmoid(both[1])
        if layer + 1 < layers:
            xg[layer + 1, t] = current.astype(jnp.bfloat16)
            sent = send_tokens(layer + 1)
        else:
            out_tok[...] = current.astype(jnp.bfloat16)
    for out in outs:
        out.wait()
    for copy in pending:
        copy.wait_send()


def body(n_tp, n_dp, *args):
    tokens, states, win = args[0], args[11], args[2]
    layers, rows, groups, entries = states.shape
    local, chans = tokens.shape[1], win.shape[2]
    own, batch = tokens.shape[0], rows * n_dp
    f32, bf16 = jnp.float32, jnp.bfloat16
    dma = pltpu.SemaphoreType.DMA
    any_spec = pl.BlockSpec(memory_space=pl.ANY)
    scratch = [pltpu.VMEM(a.shape, a.dtype) for a in args[1:]]
    scratch += [
        pltpu.VMEM((layers, n_tp, own, local), bf16),
        pltpu.VMEM((layers, 8, batch), f32),
        pltpu.VMEM((layers, n_dp, 8, batch), f32),
        pltpu.VMEM((layers, n_dp, rows, chans), f32),
        pltpu.VMEM((layers, n_dp, rows, chans), f32),
        pltpu.VMEM((layers, n_dp, rows, chans), bf16),
        pltpu.VMEM((layers, 2, n_tp, own, local), bf16),
        pltpu.VMEM((layers, 2, n_tp, own, local), bf16),
        pltpu.VMEM((layers, rows, groups, entries), f32),
        pltpu.VMEM((layers, rows, chans), f32),
        pltpu.VMEM((layers, chans, entries), f32),
        pltpu.VMEM((layers, chans, chans), f32),
        pltpu.VMEM((layers, rows, groups, entries), f32),
        dma((12,)), dma((layers,)), dma((2, layers, n_tp)), dma((2, layers, n_dp)),
        dma((2, layers, n_dp)), dma((2, layers, n_dp)), dma((2, layers, 2, n_tp)),
    ]
    return pl.pallas_call(
        functools.partial(kernel, n_tp, n_dp, float(local * n_dp)),
        out_shape=(jax.ShapeDtypeStruct(tokens.shape, bf16),
                   jax.ShapeDtypeStruct(states.shape, f32)),
        in_specs=[any_spec] * 12,
        out_specs=(pl.BlockSpec(memory_space=pltpu.VMEM), any_spec),
        scratch_shapes=scratch,
        compiler_params=pltpu.CompilerParams(
            collective_id=0, has_side_effects=True, vmem_limit_bytes=48 * 2**20),
    )(*args)


def solution(mesh):
    in_specs = (
        P("tp", "dp"),
        P(None, "dp"),
        P(None, "dp", "tp"),
        P(None, "tp", None),
        P(None, "tp", None),
        P(None, "tp"),
        P(None, "tp", None, None),
        P(None, "tp", None, None),
        P(None, "tp"),
        P(None, "tp", "dp"),
        P(None, "tp", "dp"),
        P(None, "dp", "tp", None),
    )
    out_specs = (P("tp", "dp"), P(None, "dp", "tp", None))
    run = functools.partial(body, mesh.shape["tp"], mesh.shape["dp"])
    return jax.shard_map(run, mesh=mesh, in_specs=in_specs, out_specs=out_specs, check_vma=False)
```

```python
import functools

import jax
import jax.numpy as jnp
from jax import lax
from jax.experimental import pallas as pl
from jax.experimental.pallas import tpu as pltpu
from jax.sharding import PartitionSpec as P

epsilon = 1e-06
HIGHEST = lax.Precision.HIGHEST
NT = (((1,), (1,)), ((), ()))


def iota(shape, axis):
    return lax.broadcasted_iota(jnp.int32, shape, axis)


def kernel(n_tp, n_dp, width, *refs):
    (tok, gain, win, rate, freq, step, sin, rout, skip, vw, gw, st), refs = refs[:12], refs[12:]
    (out_tok, out_st), refs = refs[:2], refs[2:]
    (tok_v, gain_v, win_v, rate_v, freq_v, step_v, sin_v, rout_v, skip_v, out_w, st_v), refs = (
        refs[:11], refs[11:])
    (xg, sq_s, sq_r, part_s, part_r, ready, prod_s, prod_r, fin_s, fin_r,
     keep_v, base_v, lift_v, mix_v, new_v,
     load_sem, out_sem, x_sem, sq_sem, part_sem, ready_sem, prod_sem, weight_sem, fin_sem) = refs
    layers, rows, groups, entries = st_v.shape
    chans = part_s.shape[-1]
    per = chans // groups
    batch = n_dp * rows
    own, half = tok_v.shape
    n_q, n_e = n_tp // 2, 2 * n_dp
    t = lax.axis_index("tp")
    d = lax.axis_index("dp")
    q, y = t // 2, lax.rem(t, 2)
    e = y * n_dp + d
    twin = 1 - y
    mine = pl.ds(pl.multiple_of(y * half, half), half)
    other = pl.ds(pl.multiple_of(twin * half, half), half)

    pairs = [
        (tok.at[:, mine], xg.at[0, t]), (tok.at[:, other], tok_v),
        (rate, rate_v), (freq, freq_v), (step, step_v), (sin, sin_v), (rout, rout_v),
        (skip, skip_v), (st, st_v), (gain.at[:, mine], gain_v)]
    for layer in range(layers):
        pairs.append((win.at[layer, mine, :], win_v.at[layer, y]))
    for layer in range(layers):
        pairs.append((vw.at[layer, :, mine], out_w.at[layer, 0, y]))
        pairs.append((gw.at[layer, :, mine], out_w.at[layer, 1, y]))
    loads = [pltpu.make_async_copy(src, dst, load_sem.at[i]) for i, (src, dst) in enumerate(pairs)]
    for load in loads:
        load.start()

    barrier = pltpu.get_barrier_semaphore()

    def greet(tp, dp):
        pl.semaphore_signal(barrier, inc=1, device_id={"tp": tp, "dp": dp},
                            device_id_type=pl.DeviceIdType.MESH)

    for k in range(1, n_tp):
        greet(lax.rem(t + k, n_tp), d)
    for k in range(1, n_dp):
        greet(t, lax.rem(d + k, n_dp))
        greet(q * 2 + twin, lax.rem(d + k, n_dp))

    pending = []

    def send(tp, dp, src, dst, sems, index):
        copy = pltpu.make_async_remote_copy(
            src_ref=src, dst_ref=dst,
            send_sem=sems.at[(0,) + index], recv_sem=sems.at[(1,) + index],
            device_id={"tp": tp, "dp": dp}, device_id_type=pl.DeviceIdType.MESH)
        copy.start()
        pending.append(copy)
        return copy

    def send_twin(src, dst, sems, index):
        return send(q * 2 + twin, d, src, dst, sems, index)

    def send_group(pick, dst, sems, layer):
        copies = []
        for k in range(1, n_e):
            to = lax.rem(e + k, n_e)
            copies.append(send(q * 2 + to // n_dp, lax.rem(to, n_dp), pick(to), dst, sems,
                               (layer, k)))
        return copies

    def send_input(layer):
        return send_twin(win.at[layer, other, :], win_v.at[layer, y], weight_sem, (layer, 0))

    def send_output(layer, which):
        return send_twin((vw, gw)[which].at[layer, :, other], out_w.at[layer, which, y],
                         weight_sem, (layer, 1 + which))

    def prepare(layer):
        half = entries // 2
        diagonal = iota((groups, groups), 0) == iota((groups, groups), 1)
        step = jnp.sum(jnp.where(diagonal, step_v[layer][None, :], 0.0), axis=1, keepdims=True)
        rate = jnp.concatenate([rate_v[layer]] * 2, axis=1)
        freq = jnp.concatenate([freq_v[layer]] * 2, axis=1)
        sign = jnp.where(iota((groups, entries), 1) < half, -1.0, 1.0)
        magnitude = jnp.exp(-rate * step)
        angle = freq * step
        keep_real = magnitude * jnp.cos(angle)
        keep_imag = magnitude * jnp.sin(angle)
        minus_one = keep_real - 1.0
        denominator = rate * rate + freq * freq
        lift_real = (-minus_one * rate + keep_imag * freq) / denominator
        lift_imag = sign * (-keep_imag * rate - minus_one * freq) / denominator
        keep_imag = sign * keep_imag

        def swap(value):
            return jnp.concatenate([value[..., half:], value[..., :half]], axis=-1)

        matrix = sin_v[layer]
        lifted = lift_real[:, None, :] * matrix + lift_imag[:, None, :] * swap(matrix)
        lifted = lifted.reshape(chans, entries)
        read = rout_v[layer].reshape(chans, entries)
        mixed = lax.dot_general(lifted, read, NT, precision=HIGHEST,
                                preferred_element_type=jnp.float32)
        first, second = iota((chans, chans), 0), iota((chans, chans), 1)
        mixed = jnp.where(first // per == second // per, mixed, 0.0)
        mixed = mixed + jnp.where(first == second, skip_v[layer][None, :], 0.0)
        old = st_v[layer]
        kept = keep_real[None] * old + keep_imag[None] * swap(old)
        base = lax.dot_general(kept.reshape(rows * groups, entries), read, NT, precision=HIGHEST,
                               preferred_element_type=jnp.float32).reshape(rows, groups, chans)
        own = iota((groups, chans), 0) == iota((groups, chans), 1) // per
        keep_v[layer] = kept
        base_v[layer] = jnp.sum(jnp.where(own[None], base, 0.0), axis=1)
        lift_v[layer] = lifted
        mix_v[layer] = mixed

    loads[0].wait()
    loads[1].wait()
    pl.semaphore_wait(barrier, n_tp - 1 + 2 * (n_dp - 1))
    sent = []
    for k in range(1, n_q):
        to = lax.rem(q + k, n_q)
        sent.append(send(to * 2 + y, d, xg.at[0, t], xg.at[0, t], x_sem, (0, 0, k)))
        sent.append(send(to * 2 + twin, d, tok_v, xg.at[0, t], x_sem, (0, 1, k)))
    sent.append(send_twin(tok_v, xg.at[0, t], x_sem, (0, 1, 0)))
    inputs = [send_input(0)]
    outputs = [[send_output(0, 0)]]
    for load in loads[2:9]:
        load.wait()
    prepare(0)
    for load in loads[9:]:
        load.wait()
    outs = []

    for layer in range(layers):
        for copy in sent:
            copy.wait_recv()
        x = xg[layer].reshape(batch, half).astype(jnp.float32)
        square = jnp.sum(x * x, axis=1, keepdims=True)
        eye = iota((batch, batch), 0) == iota((batch, batch), 1)
        line = jnp.sum(jnp.where(eye, square, 0.0), axis=0, keepdims=True)
        sq_s[layer] = jnp.broadcast_to(line, (8, batch))
        sent = send_group(lambda to: sq_s.at[layer], sq_r.at[layer, e], sq_sem, layer)
        gained = (x * gain_v[layer][None, :]).astype(jnp.bfloat16)
        inputs[layer].wait_recv()
        for i in range(2):
            part = jnp.dot(gained, win_v[layer, i], preferred_element_type=jnp.float32)
            part_s[layer, pl.ds(i * n_dp, n_dp)] = part.reshape(n_dp, rows, chans)
        sent += send_group(lambda to: part_s.at[layer, to], part_r.at[layer, e], part_sem, layer)
        if layer == 0:
            outputs[0].append(send_output(0, 1))
        total = part_s[layer, e]
        for copy in sent:
            copy.wait_recv()
        for k in range(1, n_e):
            source = lax.rem(e + n_e - k, n_e)
            total += part_r[layer, source]
            line += sq_r[layer, source][:1]
        pick = iota((rows, batch), 1) == iota((rows, batch), 0) + d * rows
        square = jnp.sum(jnp.where(pick, line, 0.0), axis=1, keepdims=True)
        drive = total * lax.rsqrt(square / width + epsilon)
        value = base_v[layer] + jnp.dot(drive, mix_v[layer], precision=HIGHEST,
                                        preferred_element_type=jnp.float32)
        ready[layer, e] = jax.nn.gelu(value).astype(jnp.bfloat16)
        sent = send_group(lambda to: ready.at[layer, e], ready.at[layer, e], ready_sem, layer)
        mask = iota((groups, chans), 0) == iota((groups, chans), 1) // per
        spread = jnp.where(mask[None], drive[:, None, :], 0.0).reshape(rows * groups, chans)
        push = jnp.dot(spread, lift_v[layer], precision=HIGHEST, preferred_element_type=jnp.float32)
        new_v[layer] = keep_v[layer] + push.reshape(rows, groups, entries)
        out = pltpu.make_async_copy(new_v.at[layer], out_st.at[layer], out_sem.at[layer])
        out.start()
        outs.append(out)
        for copy in outputs[layer] + sent:
            copy.wait_recv()
        first = ready[layer, pl.ds(0, n_dp)].reshape(batch, chans)
        second = ready[layer, pl.ds(n_dp, n_dp)].reshape(batch, chans)
        every = jnp.concatenate([first, second], axis=1)
        sent = []
        for i in range(2):
            product = jnp.dot(every, out_w[layer, i].reshape(2 * chans, half),
                              preferred_element_type=jnp.float32)
            prod_s[layer, i] = product.astype(jnp.bfloat16).reshape(n_q, 2 * own, half)
            for k in range(1, n_q):
                to = lax.rem(q + k, n_q)
                sent.append(send(to * 2 + y, d, prod_s.at[layer, i, to], prod_r.at[layer, i, q],
                                 prod_sem, (layer, i, k)))
        if layer + 1 < layers:
            inputs.append(send_input(layer + 1))
            outputs.append([send_output(layer + 1, 0), send_output(layer + 1, 1)])
            prepare(layer + 1)
        for copy in sent:
            copy.wait_recv()
        both = []
        for i in range(2):
            total = prod_s[layer, i, q].astype(jnp.float32)
            for k in range(1, n_q):
                total += prod_r[layer, i, lax.rem(q + n_q - k, n_q)].astype(jnp.float32)
            both.append(total)
        block = pl.ds(2 * q, 2)
        current = xg[layer, block].reshape(2 * own, half).astype(jnp.float32)
        current = (current + both[0] * jax.nn.sigmoid(both[1])).astype(jnp.bfloat16)
        current = current.reshape(2, own, half)
        if layer + 1 < layers:
            xg[layer + 1, block] = current
            sent = []
            for k in range(1, n_q):
                sent.append(send(lax.rem(q + k, n_q) * 2 + y, d, xg.at[layer + 1, block],
                                 xg.at[layer + 1, block], x_sem, (layer + 1, 0, k)))
        else:
            fin_s[...] = current
            copy = send_twin(fin_s.at[twin], fin_r, fin_sem, ())
            here = fin_s[y]
            copy.wait_recv()
            there = fin_r[...]
            out_tok[:, :half] = jnp.where(y == 0, here, there)
            out_tok[:, half:] = jnp.where(y == 0, there, here)
    for out in outs:
        out.wait()
    for copy in pending:
        copy.wait_send()


def body(n_tp, n_dp, *args):
    tokens, states, win = args[0], args[11], args[2]
    layers, rows, groups, entries = states.shape
    local, chans = tokens.shape[1], win.shape[2]
    own, batch, half = tokens.shape[0], rows * n_dp, local // 2
    n_q, n_e = n_tp // 2, 2 * n_dp
    f32, bf16 = jnp.float32, jnp.bfloat16
    dma = pltpu.SemaphoreType.DMA
    any_spec = pl.BlockSpec(memory_space=pl.ANY)
    scratch = [
        pltpu.VMEM((own, half), bf16),
        pltpu.VMEM((layers, half), f32),
        pltpu.VMEM((layers, 2, half, chans), bf16),
        *[pltpu.VMEM(a.shape, a.dtype) for a in args[3:9]],
        pltpu.VMEM((layers, 2, 2, chans, half), bf16),
        pltpu.VMEM(states.shape, f32),
        pltpu.VMEM((layers, n_tp, own, half), bf16),
        pltpu.VMEM((layers, 8, batch), f32),
        pltpu.VMEM((layers, n_e, 8, batch), f32),
        pltpu.VMEM((layers, n_e, rows, chans), f32),
        pltpu.VMEM((layers, n_e, rows, chans), f32),
        pltpu.VMEM((layers, n_e, rows, chans), bf16),
        pltpu.VMEM((layers, 2, n_q, 2 * own, half), bf16),
        pltpu.VMEM((layers, 2, n_q, 2 * own, half), bf16),
        pltpu.VMEM((2, own, half), bf16),
        pltpu.VMEM((own, half), bf16),
        pltpu.VMEM(states.shape, f32),
        pltpu.VMEM((layers, rows, chans), f32),
        pltpu.VMEM((layers, chans, entries), f32),
        pltpu.VMEM((layers, chans, chans), f32),
        pltpu.VMEM(states.shape, f32),
        dma((10 + 3 * layers,)), dma((layers,)), dma((2, layers, 2, n_q)), dma((2, layers, n_e)),
        dma((2, layers, n_e)), dma((2, layers, n_e)), dma((2, layers, 2, n_q)),
        dma((2, layers, 3)), dma((2,)),
    ]
    return pl.pallas_call(
        functools.partial(kernel, n_tp, n_dp, float(local * n_dp)),
        out_shape=(jax.ShapeDtypeStruct(tokens.shape, bf16),
                   jax.ShapeDtypeStruct(states.shape, f32)),
        in_specs=[any_spec] * 12,
        out_specs=(pl.BlockSpec(memory_space=pltpu.VMEM), any_spec),
        scratch_shapes=scratch,
        compiler_params=pltpu.CompilerParams(
            collective_id=0, has_side_effects=True, vmem_limit_bytes=67043328),
    )(*args)


def solution(mesh):
    in_specs = (
        P("tp", "dp"),
        P(None, "dp"),
        P(None, "dp", "tp"),
        P(None, "tp", None),
        P(None, "tp", None),
        P(None, "tp"),
        P(None, "tp", None, None),
        P(None, "tp", None, None),
        P(None, "tp"),
        P(None, "tp", "dp"),
        P(None, "tp", "dp"),
        P(None, "dp", "tp", None),
    )
    out_specs = (P("tp", "dp"), P(None, "dp", "tp", None))
    run = functools.partial(body, mesh.shape["tp"], mesh.shape["dp"])
    return jax.shard_map(run, mesh=mesh, in_specs=in_specs, out_specs=out_specs, check_vma=False)
```

```python
import functools

import jax
import jax.numpy as jnp
from jax import lax
from jax.experimental import pallas as pl
from jax.experimental.pallas import tpu as pltpu
from jax.sharding import PartitionSpec as P

epsilon = 1e-06
HIGHEST = lax.Precision.HIGHEST
NT = (((1,), (1,)), ((), ()))


def iota(shape, axis):
    return lax.broadcasted_iota(jnp.int32, shape, axis)


def kernel(n_tp, n_dp, width, *refs):
    (tok, gain, win, rate, freq, step, sin, rout, skip, vw, gw, st), refs = refs[:12], refs[12:]
    (out_tok, out_st), refs = refs[:2], refs[2:]
    (tok_v, gain_v, win_v, rate_v, freq_v, step_v, sin_v, rout_v, skip_v, out_w, st_v), refs = (
        refs[:11], refs[11:])
    (xg, sq_s, sq_r, part_v, part_s, part_r, ready, prod_s, prod_r, fin_s, fin_r,
     keep_v, base_v, lift_v, mix_v, new_v,
     load_sem, out_sem, x_sem, sq_sem, part_sem, ready_sem, prod_sem, weight_sem, fin_sem) = refs
    layers, rows, groups, entries = st_v.shape
    chans = part_s.shape[-1]
    per = chans // groups
    batch = n_dp * rows
    own, half = tok_v.shape
    n_q, n_e = n_tp // 2, 2 * n_dp
    t = lax.axis_index("tp")
    d = lax.axis_index("dp")
    q, y = t // 2, lax.rem(t, 2)
    e = y * n_dp + d
    twin = 1 - y
    mine = pl.ds(pl.multiple_of(y * half, half), half)
    other = pl.ds(pl.multiple_of(twin * half, half), half)

    pairs = [
        (tok.at[:, mine], xg.at[0, t]), (tok.at[:, other], tok_v),
        (rate, rate_v), (freq, freq_v), (step, step_v), (sin, sin_v), (rout, rout_v),
        (skip, skip_v), (st, st_v), (gain.at[:, mine], gain_v)]
    for layer in range(layers):
        pairs.append((win.at[layer, mine, :], win_v.at[layer, y]))
    for layer in range(layers):
        pairs.append((vw.at[layer, :, mine], out_w.at[layer, 0, y]))
        pairs.append((gw.at[layer, :, mine], out_w.at[layer, 1, y]))
    loads = [pltpu.make_async_copy(src, dst, load_sem.at[i]) for i, (src, dst) in enumerate(pairs)]
    for load in loads:
        load.start()

    barrier = pltpu.get_barrier_semaphore()

    def greet(tp, dp):
        pl.semaphore_signal(barrier, inc=1, device_id={"tp": tp, "dp": dp},
                            device_id_type=pl.DeviceIdType.MESH)

    for k in range(1, n_tp):
        greet(lax.rem(t + k, n_tp), d)
    for k in range(1, n_dp):
        greet(t, lax.rem(d + k, n_dp))
        greet(q * 2 + twin, lax.rem(d + k, n_dp))

    def partner(k):
        to, bit = q, 1
        while bit <= k:
            if k & bit:
                to = to + bit * (1 - 2 * lax.rem(q // bit, 2))
            bit *= 2
        return to

    hops = range(n_q - 1, 0, -1)
    pending = []

    def send(tp, dp, src, dst, sems, index):
        copy = pltpu.make_async_remote_copy(
            src_ref=src, dst_ref=dst,
            send_sem=sems.at[(0,) + index], recv_sem=sems.at[(1,) + index],
            device_id={"tp": tp, "dp": dp}, device_id_type=pl.DeviceIdType.MESH)
        copy.start()
        pending.append(copy)
        return copy

    def send_twin(src, dst, sems, index):
        return send(q * 2 + twin, d, src, dst, sems, index)

    def send_group(pick, dst, sems, layer):
        copies = []
        for k in range(1, n_e):
            to = lax.rem(e + k, n_e)
            copies.append(send(q * 2 + to // n_dp, lax.rem(to, n_dp), pick(to), dst, sems,
                               (layer, k)))
        return copies

    def send_product(layer, i, k):
        to = partner(k)
        return send(to * 2 + y, d, prod_s.at[layer, i, to], prod_r.at[layer, i, q],
                    prod_sem, (layer, i, k))

    def send_input(layer):
        return send_twin(win.at[layer, other, :], win_v.at[layer, y], weight_sem, (layer, 0))

    def send_output(layer, which):
        return send_twin((vw, gw)[which].at[layer, :, other], out_w.at[layer, which, y],
                         weight_sem, (layer, 1 + which))

    def prepare(layer):
        half = entries // 2
        diagonal = iota((groups, groups), 0) == iota((groups, groups), 1)
        step = jnp.sum(jnp.where(diagonal, step_v[layer][None, :], 0.0), axis=1, keepdims=True)
        rate = jnp.concatenate([rate_v[layer]] * 2, axis=1)
        freq = jnp.concatenate([freq_v[layer]] * 2, axis=1)
        sign = jnp.where(iota((groups, entries), 1) < half, -1.0, 1.0)
        magnitude = jnp.exp(-rate * step)
        angle = freq * step
        keep_real = magnitude * jnp.cos(angle)
        keep_imag = magnitude * jnp.sin(angle)
        minus_one = keep_real - 1.0
        denominator = rate * rate + freq * freq
        lift_real = (-minus_one * rate + keep_imag * freq) / denominator
        lift_imag = sign * (-keep_imag * rate - minus_one * freq) / denominator
        keep_imag = sign * keep_imag

        def swap(value):
            return jnp.concatenate([value[..., half:], value[..., :half]], axis=-1)

        matrix = sin_v[layer]
        lifted = lift_real[:, None, :] * matrix + lift_imag[:, None, :] * swap(matrix)
        lifted = lifted.reshape(chans, entries)
        read = rout_v[layer].reshape(chans, entries)
        mixed = lax.dot_general(lifted, read, NT, precision=HIGHEST,
                                preferred_element_type=jnp.float32)
        first, second = iota((chans, chans), 0), iota((chans, chans), 1)
        mixed = jnp.where(first // per == second // per, mixed, 0.0)
        mixed = mixed + jnp.where(first == second, skip_v[layer][None, :], 0.0)
        old = st_v[layer]
        kept = keep_real[None] * old + keep_imag[None] * swap(old)
        base = lax.dot_general(kept.reshape(rows * groups, entries), read, NT, precision=HIGHEST,
                               preferred_element_type=jnp.float32).reshape(rows, groups, chans)
        own = iota((groups, chans), 0) == iota((groups, chans), 1) // per
        keep_v[layer] = kept
        base_v[layer] = jnp.sum(jnp.where(own[None], base, 0.0), axis=1)
        lift_v[layer] = lifted
        mix_v[layer] = mixed

    loads[0].wait()
    loads[1].wait()
    pl.semaphore_wait(barrier, n_tp - 1 + 2 * (n_dp - 1))
    sent = []
    for k in hops:
        to = partner(k)
        sent.append(send(to * 2 + y, d, xg.at[0, t], xg.at[0, t], x_sem, (0, 0, k)))
        sent.append(send(to * 2 + twin, d, tok_v, xg.at[0, t], x_sem, (0, 1, k)))
    sent.append(send_twin(tok_v, xg.at[0, t], x_sem, (0, 1, 0)))
    inputs = [send_input(0)]
    outputs = [[send_output(0, 0)]]
    for load in loads[2:9]:
        load.wait()
    prepare(0)
    for load in loads[9:]:
        load.wait()
    outs = []

    for layer in range(layers):
        for copy in sent:
            copy.wait_recv()
        x = xg[layer].reshape(batch, half).astype(jnp.float32)
        square = jnp.sum(x * x, axis=1, keepdims=True)
        eye = iota((batch, batch), 0) == iota((batch, batch), 1)
        line = jnp.sum(jnp.where(eye, square, 0.0), axis=0, keepdims=True)
        sq_s[layer] = jnp.broadcast_to(line, (8, batch))
        sent = send_group(lambda to: sq_s.at[layer], sq_r.at[layer, e], sq_sem, layer)
        gained = (x * gain_v[layer][None, :]).astype(jnp.bfloat16)
        inputs[layer].wait_recv()
        for i in range(2):
            part = jnp.dot(gained, win_v[layer, i], preferred_element_type=jnp.float32)
            part_v[layer, pl.ds(i * n_dp, n_dp)] = part.reshape(n_dp, rows, chans)
            part_s[layer, pl.ds(i * n_dp, n_dp)] = (
                part.astype(jnp.bfloat16).reshape(n_dp, rows, chans))
        sent += send_group(lambda to: part_s.at[layer, to], part_r.at[layer, e], part_sem, layer)
        if layer == 0:
            outputs[0].append(send_output(0, 1))
        total = part_v[layer, e]
        for copy in sent:
            copy.wait_recv()
        for k in range(1, n_e):
            source = lax.rem(e + n_e - k, n_e)
            total += part_r[layer, source].astype(jnp.float32)
            line += sq_r[layer, source][:1]
        pick = iota((rows, batch), 1) == iota((rows, batch), 0) + d * rows
        square = jnp.sum(jnp.where(pick, line, 0.0), axis=1, keepdims=True)
        drive = total * lax.rsqrt(square / width + epsilon)
        value = base_v[layer] + jnp.dot(drive, mix_v[layer], precision=HIGHEST,
                                        preferred_element_type=jnp.float32)
        ready[layer, e] = jax.nn.gelu(value).astype(jnp.bfloat16)
        sent = send_group(lambda to: ready.at[layer, e], ready.at[layer, e], ready_sem, layer)
        mask = iota((groups, chans), 0) == iota((groups, chans), 1) // per
        spread = jnp.where(mask[None], drive[:, None, :], 0.0).reshape(rows * groups, chans)
        push = jnp.dot(spread, lift_v[layer], precision=HIGHEST, preferred_element_type=jnp.float32)
        new_v[layer] = keep_v[layer] + push.reshape(rows, groups, entries)
        out = pltpu.make_async_copy(new_v.at[layer], out_st.at[layer], out_sem.at[layer])
        out.start()
        outs.append(out)
        for copy in outputs[layer] + sent:
            copy.wait_recv()
        first = ready[layer, pl.ds(0, n_dp)].reshape(batch, chans)
        second = ready[layer, pl.ds(n_dp, n_dp)].reshape(batch, chans)
        every = jnp.concatenate([first, second], axis=1)
        sent = []
        for i in range(2):
            product = jnp.dot(every, out_w[layer, i].reshape(2 * chans, half),
                              preferred_element_type=jnp.float32)
            prod_s[layer, i] = product.astype(jnp.bfloat16).reshape(n_q, 2 * own, half)
            sent += [send_product(layer, i, k) for k in hops if k > 1]
        sent += [send_product(layer, i, 1) for i in range(2)]
        if layer + 1 < layers:
            inputs.append(send_input(layer + 1))
            outputs.append([send_output(layer + 1, 0), send_output(layer + 1, 1)])
            prepare(layer + 1)
        for copy in sent:
            copy.wait_recv()
        both = []
        for i in range(2):
            total = prod_s[layer, i, q].astype(jnp.float32)
            for k in range(1, n_q):
                total += prod_r[layer, i, partner(k)].astype(jnp.float32)
            both.append(total)
        block = pl.ds(2 * q, 2)
        current = xg[layer, block].reshape(2 * own, half).astype(jnp.float32)
        current = (current + both[0] * jax.nn.sigmoid(both[1])).astype(jnp.bfloat16)
        current = current.reshape(2, own, half)
        if layer + 1 < layers:
            xg[layer + 1, block] = current
            sent = []
            for k in hops:
                sent.append(send(partner(k) * 2 + y, d, xg.at[layer + 1, block],
                                 xg.at[layer + 1, block], x_sem, (layer + 1, 0, k)))
        else:
            fin_s[...] = current
            copy = send_twin(fin_s.at[twin], fin_r, fin_sem, ())
            here = fin_s[y]
            copy.wait_recv()
            there = fin_r[...]
            out_tok[:, :half] = jnp.where(y == 0, here, there)
            out_tok[:, half:] = jnp.where(y == 0, there, here)
    for out in outs:
        out.wait()
    for copy in pending:
        copy.wait_send()


def body(n_tp, n_dp, *args):
    tokens, states, win = args[0], args[11], args[2]
    layers, rows, groups, entries = states.shape
    local, chans = tokens.shape[1], win.shape[2]
    own, batch, half = tokens.shape[0], rows * n_dp, local // 2
    n_q, n_e = n_tp // 2, 2 * n_dp
    f32, bf16 = jnp.float32, jnp.bfloat16
    dma = pltpu.SemaphoreType.DMA
    any_spec = pl.BlockSpec(memory_space=pl.ANY)
    scratch = [
        pltpu.VMEM((own, half), bf16),
        pltpu.VMEM((layers, half), f32),
        pltpu.VMEM((layers, 2, half, chans), bf16),
        *[pltpu.VMEM(a.shape, a.dtype) for a in args[3:9]],
        pltpu.VMEM((layers, 2, 2, chans, half), bf16),
        pltpu.VMEM(states.shape, f32),
        pltpu.VMEM((layers, n_tp, own, half), bf16),
        pltpu.VMEM((layers, 8, batch), f32),
        pltpu.VMEM((layers, n_e, 8, batch), f32),
        pltpu.VMEM((layers, n_e, rows, chans), f32),
        pltpu.VMEM((layers, n_e, rows, chans), bf16),
        pltpu.VMEM((layers, n_e, rows, chans), bf16),
        pltpu.VMEM((layers, n_e, rows, chans), bf16),
        pltpu.VMEM((layers, 2, n_q, 2 * own, half), bf16),
        pltpu.VMEM((layers, 2, n_q, 2 * own, half), bf16),
        pltpu.VMEM((2, own, half), bf16),
        pltpu.VMEM((own, half), bf16),
        pltpu.VMEM(states.shape, f32),
        pltpu.VMEM((layers, rows, chans), f32),
        pltpu.VMEM((layers, chans, entries), f32),
        pltpu.VMEM((layers, chans, chans), f32),
        pltpu.VMEM(states.shape, f32),
        dma((10 + 3 * layers,)), dma((layers,)), dma((2, layers, 2, n_q)), dma((2, layers, n_e)),
        dma((2, layers, n_e)), dma((2, layers, n_e)), dma((2, layers, 2, n_q)),
        dma((2, layers, 3)), dma((2,)),
    ]
    return pl.pallas_call(
        functools.partial(kernel, n_tp, n_dp, float(local * n_dp)),
        out_shape=(jax.ShapeDtypeStruct(tokens.shape, bf16),
                   jax.ShapeDtypeStruct(states.shape, f32)),
        in_specs=[any_spec] * 12,
        out_specs=(pl.BlockSpec(memory_space=pltpu.VMEM), any_spec),
        scratch_shapes=scratch,
        compiler_params=pltpu.CompilerParams(
            collective_id=0, has_side_effects=True, vmem_limit_bytes=67043328),
    )(*args)


def solution(mesh):
    in_specs = (
        P("tp", "dp"),
        P(None, "dp"),
        P(None, "dp", "tp"),
        P(None, "tp", None),
        P(None, "tp", None),
        P(None, "tp"),
        P(None, "tp", None, None),
        P(None, "tp", None, None),
        P(None, "tp"),
        P(None, "tp", "dp"),
        P(None, "tp", "dp"),
        P(None, "dp", "tp", None),
    )
    out_specs = (P("tp", "dp"), P(None, "dp", "tp", None))
    run = functools.partial(body, mesh.shape["tp"], mesh.shape["dp"])
    return jax.shard_map(run, mesh=mesh, in_specs=in_specs, out_specs=out_specs, check_vma=False)
```

```python
import functools

import jax
import jax.numpy as jnp
from jax import lax
from jax.experimental import pallas as pl
from jax.experimental.pallas import tpu as pltpu
from jax.sharding import PartitionSpec as P

epsilon = 1e-06
HIGHEST = lax.Precision.HIGHEST
NT = (((1,), (1,)), ((), ()))


def iota(shape, axis):
    return lax.broadcasted_iota(jnp.int32, shape, axis)


def kernel(n_tp, n_dp, width, *refs):
    (tok, gain, win, rate, freq, step, sin, rout, skip, vw, gw, st), refs = refs[:12], refs[12:]
    (out_tok, out_st), refs = refs[:2], refs[2:]
    (tok_v, gain_v, win_v, rate_v, freq_v, step_v, sin_v, rout_v, skip_v, out_w, st_v), refs = (
        refs[:11], refs[11:])
    (xg, sq_s, sq_r, part_v, part_s, part_r, ready, prod_s, prod_r, last_r, fin_r,
     keep_v, base_v, lift_v, mix_v, new_v,
     load_sem, out_sem, x_sem, sq_sem, part_sem, ready_sem, prod_sem, weight_sem, fin_sem, last_sem) = refs
    layers, rows, groups, entries = st_v.shape
    chans = part_s.shape[-1]
    per = chans // groups
    batch = n_dp * rows
    own, half = tok_v.shape
    n_q, n_e = n_tp // 2, 2 * n_dp
    t = lax.axis_index("tp")
    d = lax.axis_index("dp")
    q, y = t // 2, lax.rem(t, 2)
    e = y * n_dp + d
    twin = 1 - y
    mine = pl.ds(pl.multiple_of(y * half, half), half)
    other = pl.ds(pl.multiple_of(twin * half, half), half)

    pairs = [
        (tok.at[:, mine], xg.at[0, t]), (tok.at[:, other], tok_v),
        (rate, rate_v), (freq, freq_v), (step, step_v), (sin, sin_v), (rout, rout_v),
        (skip, skip_v), (st, st_v), (gain.at[:, mine], gain_v)]
    for layer in range(layers):
        pairs.append((win.at[layer, mine, :], win_v.at[layer, y]))
    for layer in range(layers):
        pairs.append((vw.at[layer, :, mine], out_w.at[layer, 0, y]))
        pairs.append((gw.at[layer, :, mine], out_w.at[layer, 1, y]))
    loads = [pltpu.make_async_copy(src, dst, load_sem.at[i]) for i, (src, dst) in enumerate(pairs)]
    for load in loads:
        load.start()

    barrier = pltpu.get_barrier_semaphore()

    def greet(tp, dp):
        pl.semaphore_signal(barrier, inc=1, device_id={"tp": tp, "dp": dp},
                            device_id_type=pl.DeviceIdType.MESH)

    for k in range(1, n_tp):
        greet(lax.rem(t + k, n_tp), d)
    for k in range(1, n_dp):
        greet(t, lax.rem(d + k, n_dp))
        greet(q * 2 + twin, lax.rem(d + k, n_dp))

    def partner(k):
        to, bit = q, 1
        while bit <= k:
            if k & bit:
                to = to + bit * (1 - 2 * lax.rem(q // bit, 2))
            bit *= 2
        return to

    hops = range(n_q - 1, 0, -1)
    pending = []

    def send(tp, dp, src, dst, sems, index):
        copy = pltpu.make_async_remote_copy(
            src_ref=src, dst_ref=dst,
            send_sem=sems.at[(0,) + index], recv_sem=sems.at[(1,) + index],
            device_id={"tp": tp, "dp": dp}, device_id_type=pl.DeviceIdType.MESH)
        copy.start()
        pending.append(copy)
        return copy

    def send_twin(src, dst, sems, index):
        return send(q * 2 + twin, d, src, dst, sems, index)

    def send_group(pick, dst, sems, layer):
        copies = []
        for k in range(1, n_e):
            to = lax.rem(e + k, n_e)
            copies.append(send(q * 2 + to // n_dp, lax.rem(to, n_dp), pick(to), dst, sems,
                               (layer, k)))
        return copies

    def send_product(layer, i, k):
        to = partner(k)
        return send(to * 2 + y, d, prod_s.at[layer, i, to], prod_r.at[layer, i, q],
                    prod_sem, (layer, i, k))

    def send_last(i, cross, k):
        row = twin if cross else y
        to = partner(k)
        return send(to * 2 + row, d, prod_s.at[layers - 1, i, to, row], last_r.at[i, t],
                    last_sem, (i, cross, k))

    def send_input(layer):
        return send_twin(win.at[layer, other, :], win_v.at[layer, y], weight_sem, (layer, 0))

    def send_output(layer, which):
        return send_twin((vw, gw)[which].at[layer, :, other], out_w.at[layer, which, y],
                         weight_sem, (layer, 1 + which))

    def prepare(layer):
        half = entries // 2
        diagonal = iota((groups, groups), 0) == iota((groups, groups), 1)
        step = jnp.sum(jnp.where(diagonal, step_v[layer][None, :], 0.0), axis=1, keepdims=True)
        rate = jnp.concatenate([rate_v[layer]] * 2, axis=1)
        freq = jnp.concatenate([freq_v[layer]] * 2, axis=1)
        sign = jnp.where(iota((groups, entries), 1) < half, -1.0, 1.0)
        magnitude = jnp.exp(-rate * step)
        angle = freq * step
        keep_real = magnitude * jnp.cos(angle)
        keep_imag = magnitude * jnp.sin(angle)
        minus_one = keep_real - 1.0
        denominator = rate * rate + freq * freq
        lift_real = (-minus_one * rate + keep_imag * freq) / denominator
        lift_imag = sign * (-keep_imag * rate - minus_one * freq) / denominator
        keep_imag = sign * keep_imag

        def swap(value):
            return jnp.concatenate([value[..., half:], value[..., :half]], axis=-1)

        matrix = sin_v[layer]
        lifted = lift_real[:, None, :] * matrix + lift_imag[:, None, :] * swap(matrix)
        lifted = lifted.reshape(chans, entries)
        read = rout_v[layer].reshape(chans, entries)
        mixed = lax.dot_general(lifted, read, NT, precision=HIGHEST,
                                preferred_element_type=jnp.float32)
        first, second = iota((chans, chans), 0), iota((chans, chans), 1)
        mixed = jnp.where(first // per == second // per, mixed, 0.0)
        mixed = mixed + jnp.where(first == second, skip_v[layer][None, :], 0.0)
        old = st_v[layer]
        kept = keep_real[None] * old + keep_imag[None] * swap(old)
        base = lax.dot_general(kept.reshape(rows * groups, entries), read, NT, precision=HIGHEST,
                               preferred_element_type=jnp.float32).reshape(rows, groups, chans)
        own = iota((groups, chans), 0) == iota((groups, chans), 1) // per
        keep_v[layer] = kept
        base_v[layer] = jnp.sum(jnp.where(own[None], base, 0.0), axis=1)
        lift_v[layer] = lifted
        mix_v[layer] = mixed

    loads[0].wait()
    loads[1].wait()
    pl.semaphore_wait(barrier, n_tp - 1 + 2 * (n_dp - 1))
    sent = []
    for k in hops:
        to = partner(k)
        sent.append(send(to * 2 + y, d, xg.at[0, t], xg.at[0, t], x_sem, (0, 0, k)))
        sent.append(send(to * 2 + twin, d, tok_v, xg.at[0, t], x_sem, (0, 1, k)))
    sent.append(send_twin(tok_v, xg.at[0, t], x_sem, (0, 1, 0)))
    inputs = [send_input(0)]
    outputs = [[send_output(0, 0)]]
    for load in loads[2:9]:
        load.wait()
    prepare(0)
    for load in loads[9:]:
        load.wait()
    outs = []

    for layer in range(layers):
        for copy in sent:
            copy.wait_recv()
        x = xg[layer].reshape(batch, half).astype(jnp.float32)
        square = jnp.sum(x * x, axis=1, keepdims=True)
        eye = iota((batch, batch), 0) == iota((batch, batch), 1)
        line = jnp.sum(jnp.where(eye, square, 0.0), axis=0, keepdims=True)
        sq_s[layer] = jnp.broadcast_to(line, (8, batch))
        sent = send_group(lambda to: sq_s.at[layer], sq_r.at[layer, e], sq_sem, layer)
        gained = (x * gain_v[layer][None, :]).astype(jnp.bfloat16)
        inputs[layer].wait_recv()
        for i in range(2):
            part = jnp.dot(gained, win_v[layer, i], preferred_element_type=jnp.float32)
            part_v[layer, pl.ds(i * n_dp, n_dp)] = part.reshape(n_dp, rows, chans)
            part_s[layer, pl.ds(i * n_dp, n_dp)] = (
                part.astype(jnp.bfloat16).reshape(n_dp, rows, chans))
        sent += send_group(lambda to: part_s.at[layer, to], part_r.at[layer, e], part_sem, layer)
        if layer == 0:
            outputs[0].append(send_output(0, 1))
        total = part_v[layer, e]
        for copy in sent:
            copy.wait_recv()
        for k in range(1, n_e):
            source = lax.rem(e + n_e - k, n_e)
            total += part_r[layer, source].astype(jnp.float32)
            line += sq_r[layer, source][:1]
        pick = iota((rows, batch), 1) == iota((rows, batch), 0) + d * rows
        square = jnp.sum(jnp.where(pick, line, 0.0), axis=1, keepdims=True)
        drive = total * lax.rsqrt(square / width + epsilon)
        value = base_v[layer] + jnp.dot(drive, mix_v[layer], precision=HIGHEST,
                                        preferred_element_type=jnp.float32)
        ready[layer, e] = jax.nn.gelu(value).astype(jnp.bfloat16)
        sent = send_group(lambda to: ready.at[layer, e], ready.at[layer, e], ready_sem, layer)
        mask = iota((groups, chans), 0) == iota((groups, chans), 1) // per
        spread = jnp.where(mask[None], drive[:, None, :], 0.0).reshape(rows * groups, chans)
        push = jnp.dot(spread, lift_v[layer], precision=HIGHEST, preferred_element_type=jnp.float32)
        new_v[layer] = keep_v[layer] + push.reshape(rows, groups, entries)
        out = pltpu.make_async_copy(new_v.at[layer], out_st.at[layer], out_sem.at[layer])
        out.start()
        outs.append(out)
        for copy in outputs[layer] + sent:
            copy.wait_recv()
        first = ready[layer, pl.ds(0, n_dp)].reshape(batch, chans)
        second = ready[layer, pl.ds(n_dp, n_dp)].reshape(batch, chans)
        every = jnp.concatenate([first, second], axis=1)
        sent = []
        for i in range(2):
            product = jnp.dot(every, out_w[layer, i].reshape(2 * chans, half),
                              preferred_element_type=jnp.float32)
            prod_s[layer, i] = product.astype(jnp.bfloat16).reshape(n_q, 2, own, half)
            if layer + 1 < layers:
                sent += [send_product(layer, i, k) for k in hops if k > 1]
            else:
                sent += [send_last(i, c, k) for k in hops if k > 1 for c in (1, 0)]
        if layer + 1 < layers:
            sent += [send_product(layer, i, 1) for i in range(2)]
        else:
            sent += [send_last(i, c, k) for c, k in ((1, 1), (0, 1), (1, 0)) for i in range(2)]
        if layer + 1 < layers:
            inputs.append(send_input(layer + 1))
            outputs.append([send_output(layer + 1, 0), send_output(layer + 1, 1)])
            prepare(layer + 1)
        for copy in sent:
            copy.wait_recv()
        f32 = jnp.float32
        if layer + 1 < layers:
            both = []
            for i in range(2):
                total = prod_s[layer, i, q].astype(f32)
                for k in range(1, n_q):
                    total += prod_r[layer, i, partner(k)].astype(f32)
                both.append(total)
            block = pl.ds(2 * q, 2)
            current = xg[layer, block].astype(f32) + both[0] * jax.nn.sigmoid(both[1])
            xg[layer + 1, block] = current.astype(jnp.bfloat16)
            sent = []
            for k in hops:
                sent.append(send(partner(k) * 2 + y, d, xg.at[layer + 1, block],
                                 xg.at[layer + 1, block], x_sem, (layer + 1, 0, k)))
            if layer + 2 == layers:
                rest = send_twin(xg.at[layer + 1, q * 2 + twin], fin_r, fin_sem, ())
        else:
            rest.wait_recv()
            same, cross = [], []
            for i in range(2):
                total = prod_s[layer, i, q, y].astype(f32)
                for k in range(1, n_q):
                    total += last_r[i, partner(k) * 2 + y].astype(f32)
                same.append(total)
                total = last_r[i, q * 2 + twin].astype(f32)
                for k in range(1, n_q):
                    total += last_r[i, partner(k) * 2 + twin].astype(f32)
                cross.append(total)
            here = xg[layer, t].astype(f32) + same[0] * jax.nn.sigmoid(same[1])
            there = fin_r[...].astype(f32) + cross[0] * jax.nn.sigmoid(cross[1])
            out_tok[:, :half] = jnp.where(y == 0, here, there).astype(jnp.bfloat16)
            out_tok[:, half:] = jnp.where(y == 0, there, here).astype(jnp.bfloat16)
    for out in outs:
        out.wait()
    for copy in pending:
        copy.wait_send()


def body(n_tp, n_dp, *args):
    tokens, states, win = args[0], args[11], args[2]
    layers, rows, groups, entries = states.shape
    local, chans = tokens.shape[1], win.shape[2]
    own, batch, half = tokens.shape[0], rows * n_dp, local // 2
    n_q, n_e = n_tp // 2, 2 * n_dp
    f32, bf16 = jnp.float32, jnp.bfloat16
    dma = pltpu.SemaphoreType.DMA
    any_spec = pl.BlockSpec(memory_space=pl.ANY)
    scratch = [
        pltpu.VMEM((own, half), bf16),
        pltpu.VMEM((layers, half), f32),
        pltpu.VMEM((layers, 2, half, chans), bf16),
        *[pltpu.VMEM(a.shape, a.dtype) for a in args[3:9]],
        pltpu.VMEM((layers, 2, 2, chans, half), bf16),
        pltpu.VMEM(states.shape, f32),
        pltpu.VMEM((layers, n_tp, own, half), bf16),
        pltpu.VMEM((layers, 8, batch), f32),
        pltpu.VMEM((layers, n_e, 8, batch), f32),
        pltpu.VMEM((layers, n_e, rows, chans), f32),
        pltpu.VMEM((layers, n_e, rows, chans), bf16),
        pltpu.VMEM((layers, n_e, rows, chans), bf16),
        pltpu.VMEM((layers, n_e, rows, chans), bf16),
        pltpu.VMEM((layers, 2, n_q, 2, own, half), bf16),
        pltpu.VMEM((layers - 1, 2, n_q, 2, own, half), bf16),
        pltpu.VMEM((2, n_tp, own, half), bf16),
        pltpu.VMEM((own, half), bf16),
        pltpu.VMEM(states.shape, f32),
        pltpu.VMEM((layers, rows, chans), f32),
        pltpu.VMEM((layers, chans, entries), f32),
        pltpu.VMEM((layers, chans, chans), f32),
        pltpu.VMEM(states.shape, f32),
        dma((10 + 3 * layers,)), dma((layers,)), dma((2, layers, 2, n_q)), dma((2, layers, n_e)),
        dma((2, layers, n_e)), dma((2, layers, n_e)), dma((2, layers, 2, n_q)),
        dma((2, layers, 3)), dma((2,)), dma((2, 2, 2, n_q)),
    ]
    return pl.pallas_call(
        functools.partial(kernel, n_tp, n_dp, float(local * n_dp)),
        out_shape=(jax.ShapeDtypeStruct(tokens.shape, bf16),
                   jax.ShapeDtypeStruct(states.shape, f32)),
        in_specs=[any_spec] * 12,
        out_specs=(pl.BlockSpec(memory_space=pltpu.VMEM), any_spec),
        scratch_shapes=scratch,
        compiler_params=pltpu.CompilerParams(
            collective_id=0, has_side_effects=True, vmem_limit_bytes=67043328),
    )(*args)


def solution(mesh):
    in_specs = (
        P("tp", "dp"),
        P(None, "dp"),
        P(None, "dp", "tp"),
        P(None, "tp", None),
        P(None, "tp", None),
        P(None, "tp"),
        P(None, "tp", None, None),
        P(None, "tp", None, None),
        P(None, "tp"),
        P(None, "tp", "dp"),
        P(None, "tp", "dp"),
        P(None, "dp", "tp", None),
    )
    out_specs = (P("tp", "dp"), P(None, "dp", "tp", None))
    run = functools.partial(body, mesh.shape["tp"], mesh.shape["dp"])
    return jax.shard_map(run, mesh=mesh, in_specs=in_specs, out_specs=out_specs, check_vma=False)
```

```python
import functools

import jax
import jax.numpy as jnp
from jax import lax
from jax.experimental import pallas as pl
from jax.experimental.pallas import tpu as pltpu
from jax.sharding import PartitionSpec as P

epsilon = 1e-06
HIGHEST = lax.Precision.HIGHEST
NT = (((1,), (1,)), ((), ()))


def iota(shape, axis):
    return lax.broadcasted_iota(jnp.int32, shape, axis)


def kernel(n_tp, n_dp, width, *refs):
    (tok, gain, win, rate, freq, step, sin, rout, skip, vw, gw, st), refs = refs[:12], refs[12:]
    (out_tok, out_st), refs = refs[:2], refs[2:]
    (tok_v, gain_v, win_v, rate_v, freq_v, step_v, sin_v, rout_v, skip_v, out_w, st_v), refs = (
        refs[:11], refs[11:])
    (xg, sq_s, sq_r, part_v, part_s, part_r, ready, prod_s, prod_r, last_r, fin_r, relay_s, relay_r,
     keep_v, base_v, lift_v, mix_v, new_v,
     load_sem, out_sem, x_sem, sq_sem, part_sem, ready_sem, prod_sem, weight_sem, fin_sem, last_sem, relay_sem) = refs
    layers, rows, groups, entries = st_v.shape
    chans = part_s.shape[-1]
    per = chans // groups
    batch = n_dp * rows
    own, half = tok_v.shape
    n_q, n_e = n_tp // 2, 2 * n_dp
    t = lax.axis_index("tp")
    d = lax.axis_index("dp")
    q, y = t // 2, lax.rem(t, 2)
    e = y * n_dp + d
    twin = 1 - y
    mine = pl.ds(pl.multiple_of(y * half, half), half)
    other = pl.ds(pl.multiple_of(twin * half, half), half)

    pairs = [
        (tok.at[:, mine], xg.at[0, t]), (tok.at[:, other], tok_v),
        (rate, rate_v), (freq, freq_v), (step, step_v), (sin, sin_v), (rout, rout_v),
        (skip, skip_v), (st, st_v), (gain.at[:, mine], gain_v)]
    for layer in range(layers):
        pairs.append((win.at[layer, mine, :], win_v.at[layer, y]))
    for layer in range(layers):
        pairs.append((vw.at[layer, :, mine], out_w.at[layer, 0, y]))
        pairs.append((gw.at[layer, :, mine], out_w.at[layer, 1, y]))
    loads = [pltpu.make_async_copy(src, dst, load_sem.at[i]) for i, (src, dst) in enumerate(pairs)]
    for load in loads:
        load.start()

    barrier = pltpu.get_barrier_semaphore()

    def greet(tp, dp):
        pl.semaphore_signal(barrier, inc=1, device_id={"tp": tp, "dp": dp},
                            device_id_type=pl.DeviceIdType.MESH)

    for k in range(1, n_tp):
        greet(lax.rem(t + k, n_tp), d)
    for k in range(1, n_dp):
        greet(t, lax.rem(d + k, n_dp))
        greet(q * 2 + twin, lax.rem(d + k, n_dp))

    def partner(k):
        to, bit = q, 1
        while bit <= k:
            if k & bit:
                to = to + bit * (1 - 2 * lax.rem(q // bit, 2))
            bit *= 2
        return to

    hops = range(n_q - 1, 0, -1)
    pending = []

    def send(tp, dp, src, dst, sems, index):
        copy = pltpu.make_async_remote_copy(
            src_ref=src, dst_ref=dst,
            send_sem=sems.at[(0,) + index], recv_sem=sems.at[(1,) + index],
            device_id={"tp": tp, "dp": dp}, device_id_type=pl.DeviceIdType.MESH)
        copy.start()
        pending.append(copy)
        return copy

    def send_twin(src, dst, sems, index):
        return send(q * 2 + twin, d, src, dst, sems, index)

    def send_group(pick, dst, sems, layer):
        copies = []
        for k in range(1, n_e):
            to = lax.rem(e + k, n_e)
            copies.append(send(q * 2 + to // n_dp, lax.rem(to, n_dp), pick(to), dst, sems,
                               (layer, k)))
        return copies

    far = range(n_q - 1, 1, -2)
    heard = (1,) + tuple(k - 1 for k in far)

    def send_relay(layer, i, k):
        return send(partner(1) * 2 + y, d, prod_s.at[layer, i, partner(k)],
                    relay_r.at[layer, i, k // 2], relay_sem, (layer, i, k // 2))

    def send_product(layer, i, k, source):
        to = partner(k)
        return send(to * 2 + y, d, source, prod_r.at[layer, i, q],
                    prod_sem, (layer, i, k))

    def send_last(i, cross, k):
        row = twin if cross else y
        to = partner(k)
        return send(to * 2 + row, d, prod_s.at[layers - 1, i, to, row], last_r.at[i, t],
                    last_sem, (i, cross, k))

    def send_input(layer):
        return send_twin(win.at[layer, other, :], win_v.at[layer, y], weight_sem, (layer, 0))

    def send_output(layer, which):
        return send_twin((vw, gw)[which].at[layer, :, other], out_w.at[layer, which, y],
                         weight_sem, (layer, 1 + which))

    def prepare(layer):
        half = entries // 2
        diagonal = iota((groups, groups), 0) == iota((groups, groups), 1)
        step = jnp.sum(jnp.where(diagonal, step_v[layer][None, :], 0.0), axis=1, keepdims=True)
        rate = jnp.concatenate([rate_v[layer]] * 2, axis=1)
        freq = jnp.concatenate([freq_v[layer]] * 2, axis=1)
        sign = jnp.where(iota((groups, entries), 1) < half, -1.0, 1.0)
        magnitude = jnp.exp(-rate * step)
        angle = freq * step
        keep_real = magnitude * jnp.cos(angle)
        keep_imag = magnitude * jnp.sin(angle)
        minus_one = keep_real - 1.0
        denominator = rate * rate + freq * freq
        lift_real = (-minus_one * rate + keep_imag * freq) / denominator
        lift_imag = sign * (-keep_imag * rate - minus_one * freq) / denominator
        keep_imag = sign * keep_imag

        def swap(value):
            return jnp.concatenate([value[..., half:], value[..., :half]], axis=-1)

        matrix = sin_v[layer]
        lifted = lift_real[:, None, :] * matrix + lift_imag[:, None, :] * swap(matrix)
        lifted = lifted.reshape(chans, entries)
        read = rout_v[layer].reshape(chans, entries)
        mixed = lax.dot_general(lifted, read, NT, precision=HIGHEST,
                                preferred_element_type=jnp.float32)
        first, second = iota((chans, chans), 0), iota((chans, chans), 1)
        mixed = jnp.where(first // per == second // per, mixed, 0.0)
        mixed = mixed + jnp.where(first == second, skip_v[layer][None, :], 0.0)
        old = st_v[layer]
        kept = keep_real[None] * old + keep_imag[None] * swap(old)
        base = lax.dot_general(kept.reshape(rows * groups, entries), read, NT, precision=HIGHEST,
                               preferred_element_type=jnp.float32).reshape(rows, groups, chans)
        own = iota((groups, chans), 0) == iota((groups, chans), 1) // per
        keep_v[layer] = kept
        base_v[layer] = jnp.sum(jnp.where(own[None], base, 0.0), axis=1)
        lift_v[layer] = lifted
        mix_v[layer] = mixed

    loads[0].wait()
    loads[1].wait()
    pl.semaphore_wait(barrier, n_tp - 1 + 2 * (n_dp - 1))
    sent = []
    for k in hops:
        to = partner(k)
        sent.append(send(to * 2 + y, d, xg.at[0, t], xg.at[0, t], x_sem, (0, 0, k)))
        sent.append(send(to * 2 + twin, d, tok_v, xg.at[0, t], x_sem, (0, 1, k)))
    sent.append(send_twin(tok_v, xg.at[0, t], x_sem, (0, 1, 0)))
    inputs = [send_input(0)]
    outputs = [[send_output(0, 0)]]
    for load in loads[2:9]:
        load.wait()
    prepare(0)
    for load in loads[9:]:
        load.wait()
    outs = []

    for layer in range(layers):
        for copy in sent:
            copy.wait_recv()
        x = xg[layer].reshape(batch, half).astype(jnp.float32)
        square = jnp.sum(x * x, axis=1, keepdims=True)
        eye = iota((batch, batch), 0) == iota((batch, batch), 1)
        line = jnp.sum(jnp.where(eye, square, 0.0), axis=0, keepdims=True)
        sq_s[layer] = jnp.broadcast_to(line, (8, batch))
        sent = send_group(lambda to: sq_s.at[layer], sq_r.at[layer, e], sq_sem, layer)
        gained = (x * gain_v[layer][None, :]).astype(jnp.bfloat16)
        inputs[layer].wait_recv()
        for i in range(2):
            part = jnp.dot(gained, win_v[layer, i], preferred_element_type=jnp.float32)
            part_v[layer, pl.ds(i * n_dp, n_dp)] = part.reshape(n_dp, rows, chans)
            part_s[layer, pl.ds(i * n_dp, n_dp)] = (
                part.astype(jnp.bfloat16).reshape(n_dp, rows, chans))
        sent += send_group(lambda to: part_s.at[layer, to], part_r.at[layer, e], part_sem, layer)
        if layer == 0:
            outputs[0].append(send_output(0, 1))
        total = part_v[layer, e]
        for copy in sent:
            copy.wait_recv()
        for k in range(1, n_e):
            source = lax.rem(e + n_e - k, n_e)
            total += part_r[layer, source].astype(jnp.float32)
            line += sq_r[layer, source][:1]
        pick = iota((rows, batch), 1) == iota((rows, batch), 0) + d * rows
        square = jnp.sum(jnp.where(pick, line, 0.0), axis=1, keepdims=True)
        drive = total * lax.rsqrt(square / width + epsilon)
        value = base_v[layer] + jnp.dot(drive, mix_v[layer], precision=HIGHEST,
                                        preferred_element_type=jnp.float32)
        ready[layer, e] = jax.nn.gelu(value).astype(jnp.bfloat16)
        sent = send_group(lambda to: ready.at[layer, e], ready.at[layer, e], ready_sem, layer)
        mask = iota((groups, chans), 0) == iota((groups, chans), 1) // per
        spread = jnp.where(mask[None], drive[:, None, :], 0.0).reshape(rows * groups, chans)
        push = jnp.dot(spread, lift_v[layer], precision=HIGHEST, preferred_element_type=jnp.float32)
        new_v[layer] = keep_v[layer] + push.reshape(rows, groups, entries)
        out = pltpu.make_async_copy(new_v.at[layer], out_st.at[layer], out_sem.at[layer])
        out.start()
        outs.append(out)
        for copy in outputs[layer] + sent:
            copy.wait_recv()
        first = ready[layer, pl.ds(0, n_dp)].reshape(batch, chans)
        second = ready[layer, pl.ds(n_dp, n_dp)].reshape(batch, chans)
        every = jnp.concatenate([first, second], axis=1)
        sent, relays = [], []
        for i in range(2):
            product = jnp.dot(every, out_w[layer, i].reshape(2 * chans, half),
                              preferred_element_type=jnp.float32)
            prod_s[layer, i] = product.astype(jnp.bfloat16).reshape(n_q, 2, own, half)
            if layer + 1 < layers:
                relays.append([send_relay(layer, i, k) for k in far])
            else:
                sent += [send_last(i, c, k) for k in hops if k > 1 for c in (1, 0)]
        if layer + 1 < layers:
            sent += [send_product(layer, i, 1, prod_s.at[layer, i, partner(1)]) for i in range(2)]
            for i in range(2):
                for copy, k in zip(relays[i], far):
                    copy.wait_recv()
                    joined = (prod_s[layer, i, partner(k - 1)].astype(jnp.float32)
                              + relay_r[layer, i, k // 2].astype(jnp.float32))
                    relay_s[layer, i, k // 2] = joined.astype(jnp.bfloat16)
                    sent.append(send_product(layer, i, k - 1, relay_s.at[layer, i, k // 2]))
        else:
            sent += [send_last(i, c, k) for c, k in ((1, 1), (0, 1), (1, 0)) for i in range(2)]
        if layer + 1 < layers:
            inputs.append(send_input(layer + 1))
            outputs.append([send_output(layer + 1, 0), send_output(layer + 1, 1)])
            prepare(layer + 1)
        for copy in sent:
            copy.wait_recv()
        f32 = jnp.float32
        if layer + 1 < layers:
            both = []
            for i in range(2):
                total = prod_s[layer, i, q].astype(f32)
                for k in heard:
                    total += prod_r[layer, i, partner(k)].astype(f32)
                both.append(total)
            block = pl.ds(2 * q, 2)
            current = xg[layer, block].astype(f32) + both[0] * jax.nn.sigmoid(both[1])
            xg[layer + 1, block] = current.astype(jnp.bfloat16)
            sent = []
            for k in hops:
                sent.append(send(partner(k) * 2 + y, d, xg.at[layer + 1, block],
                                 xg.at[layer + 1, block], x_sem, (layer + 1, 0, k)))
            if layer + 2 == layers:
                rest = send_twin(xg.at[layer + 1, q * 2 + twin], fin_r, fin_sem, ())
        else:
            rest.wait_recv()
            same, cross = [], []
            for i in range(2):
                total = prod_s[layer, i, q, y].astype(f32)
                for k in range(1, n_q):
                    total += last_r[i, partner(k) * 2 + y].astype(f32)
                same.append(total)
                total = last_r[i, q * 2 + twin].astype(f32)
                for k in range(1, n_q):
                    total += last_r[i, partner(k) * 2 + twin].astype(f32)
                cross.append(total)
            here = xg[layer, t].astype(f32) + same[0] * jax.nn.sigmoid(same[1])
            there = fin_r[...].astype(f32) + cross[0] * jax.nn.sigmoid(cross[1])
            out_tok[:, :half] = jnp.where(y == 0, here, there).astype(jnp.bfloat16)
            out_tok[:, half:] = jnp.where(y == 0, there, here).astype(jnp.bfloat16)
    for out in outs:
        out.wait()
    for copy in pending:
        copy.wait_send()


def body(n_tp, n_dp, *args):
    tokens, states, win = args[0], args[11], args[2]
    layers, rows, groups, entries = states.shape
    local, chans = tokens.shape[1], win.shape[2]
    own, batch, half = tokens.shape[0], rows * n_dp, local // 2
    n_q, n_e = n_tp // 2, 2 * n_dp
    f32, bf16 = jnp.float32, jnp.bfloat16
    dma = pltpu.SemaphoreType.DMA
    any_spec = pl.BlockSpec(memory_space=pl.ANY)
    scratch = [
        pltpu.VMEM((own, half), bf16),
        pltpu.VMEM((layers, half), f32),
        pltpu.VMEM((layers, 2, half, chans), bf16),
        *[pltpu.VMEM(a.shape, a.dtype) for a in args[3:9]],
        pltpu.VMEM((layers, 2, 2, chans, half), bf16),
        pltpu.VMEM(states.shape, f32),
        pltpu.VMEM((layers, n_tp, own, half), bf16),
        pltpu.VMEM((layers, 8, batch), f32),
        pltpu.VMEM((layers, n_e, 8, batch), f32),
        pltpu.VMEM((layers, n_e, rows, chans), f32),
        pltpu.VMEM((layers, n_e, rows, chans), bf16),
        pltpu.VMEM((layers, n_e, rows, chans), bf16),
        pltpu.VMEM((layers, n_e, rows, chans), bf16),
        pltpu.VMEM((layers, 2, n_q, 2, own, half), bf16),
        pltpu.VMEM((layers - 1, 2, n_q, 2, own, half), bf16),
        pltpu.VMEM((2, n_tp, own, half), bf16),
        pltpu.VMEM((own, half), bf16),
        *[pltpu.VMEM((layers - 1, 2, n_q // 2, 2, own, half), bf16)] * 2,
        pltpu.VMEM(states.shape, f32),
        pltpu.VMEM((layers, rows, chans), f32),
        pltpu.VMEM((layers, chans, entries), f32),
        pltpu.VMEM((layers, chans, chans), f32),
        pltpu.VMEM(states.shape, f32),
        dma((10 + 3 * layers,)), dma((layers,)), dma((2, layers, 2, n_q)), dma((2, layers, n_e)),
        dma((2, layers, n_e)), dma((2, layers, n_e)), dma((2, layers, 2, n_q)),
        dma((2, layers, 3)), dma((2,)), dma((2, 2, 2, n_q)),
        dma((2, layers - 1, 2, n_q // 2)),
    ]
    return pl.pallas_call(
        functools.partial(kernel, n_tp, n_dp, float(local * n_dp)),
        out_shape=(jax.ShapeDtypeStruct(tokens.shape, bf16),
                   jax.ShapeDtypeStruct(states.shape, f32)),
        in_specs=[any_spec] * 12,
        out_specs=(pl.BlockSpec(memory_space=pltpu.VMEM), any_spec),
        scratch_shapes=scratch,
        compiler_params=pltpu.CompilerParams(
            collective_id=0, has_side_effects=True, vmem_limit_bytes=67043328),
    )(*args)


def solution(mesh):
    in_specs = (
        P("tp", "dp"),
        P(None, "dp"),
        P(None, "dp", "tp"),
        P(None, "tp", None),
        P(None, "tp", None),
        P(None, "tp"),
        P(None, "tp", None, None),
        P(None, "tp", None, None),
        P(None, "tp"),
        P(None, "tp", "dp"),
        P(None, "tp", "dp"),
        P(None, "dp", "tp", None),
    )
    out_specs = (P("tp", "dp"), P(None, "dp", "tp", None))
    run = functools.partial(body, mesh.shape["tp"], mesh.shape["dp"])
    return jax.shard_map(run, mesh=mesh, in_specs=in_specs, out_specs=out_specs, check_vma=False)
```

```python
import functools

import jax
import jax.numpy as jnp
from jax import lax
from jax.experimental import pallas as pl
from jax.experimental.pallas import tpu as pltpu
from jax.sharding import PartitionSpec as P

epsilon = 1e-06
HIGHEST = lax.Precision.HIGHEST
NT = (((1,), (1,)), ((), ()))


def iota(shape, axis):
    return lax.broadcasted_iota(jnp.int32, shape, axis)


def kernel(n_tp, n_dp, width, *refs):
    (tok, gain, win, rate, freq, step, sin, rout, skip, vw, gw, st), refs = refs[:12], refs[12:]
    (out_tok, out_st), refs = refs[:2], refs[2:]
    (tok_v, gain_v, win_v, rate_v, freq_v, step_v, sin_v, rout_v, skip_v, out_w, st_v), refs = (
        refs[:11], refs[11:])
    (xg, sq_s, sq_r, part_v, part_s, part_r, ready, prod_s, prod_r, last_r, fin_r, relay_s, relay_r,
     keep_v, base_v, lift_v, mix_v, new_v,
     load_sem, out_sem, x_sem, sq_sem, part_sem, ready_sem, prod_sem, weight_sem, fin_sem, last_sem, relay_sem) = refs
    layers, rows, groups, entries = st_v.shape
    chans = part_s.shape[-1]
    per = chans // groups
    batch = n_dp * rows
    own, half = tok_v.shape
    n_q, n_e = n_tp // 2, 2 * n_dp
    t = lax.axis_index("tp")
    d = lax.axis_index("dp")
    q, y = t // 2, lax.rem(t, 2)
    e = y * n_dp + d
    twin = 1 - y
    mine = pl.ds(pl.multiple_of(y * half, half), half)
    other = pl.ds(pl.multiple_of(twin * half, half), half)

    pairs = [
        (tok.at[:, mine], xg.at[0, t]), (tok.at[:, other], tok_v),
        (rate, rate_v), (freq, freq_v), (step, step_v), (sin, sin_v), (rout, rout_v),
        (skip, skip_v), (st, st_v), (gain.at[:, mine], gain_v)]
    for layer in range(layers):
        pairs.append((win.at[layer, mine, :], win_v.at[layer, y]))
    for layer in range(layers):
        pairs.append((vw.at[layer, :, mine], out_w.at[layer, 0, y]))
        pairs.append((gw.at[layer, :, mine], out_w.at[layer, 1, y]))
    loads = [pltpu.make_async_copy(src, dst, load_sem.at[i]) for i, (src, dst) in enumerate(pairs)]
    for load in loads:
        load.start()

    barrier = pltpu.get_barrier_semaphore()

    def greet(tp, dp):
        pl.semaphore_signal(barrier, inc=1, device_id={"tp": tp, "dp": dp},
                            device_id_type=pl.DeviceIdType.MESH)

    for k in range(1, n_tp):
        greet(lax.rem(t + k, n_tp), d)
    for k in range(1, n_dp):
        greet(t, lax.rem(d + k, n_dp))
        greet(q * 2 + twin, lax.rem(d + k, n_dp))

    def partner(k):
        to, bit = q, 1
        while bit <= k:
            if k & bit:
                to = to + bit * (1 - 2 * lax.rem(q // bit, 2))
            bit *= 2
        return to

    hops = range(n_q - 1, 0, -1)
    pending = []

    def send(tp, dp, src, dst, sems, index):
        copy = pltpu.make_async_remote_copy(
            src_ref=src, dst_ref=dst,
            send_sem=sems.at[(0,) + index], recv_sem=sems.at[(1,) + index],
            device_id={"tp": tp, "dp": dp}, device_id_type=pl.DeviceIdType.MESH)
        copy.start()
        pending.append(copy)
        return copy

    def send_twin(src, dst, sems, index):
        return send(q * 2 + twin, d, src, dst, sems, index)

    def send_group(pick, dst, sems, layer):
        copies = []
        for k in range(1, n_e):
            to = lax.rem(e + k, n_e)
            copies.append(send(q * 2 + to // n_dp, lax.rem(to, n_dp), pick(to), dst, sems,
                               (layer, k)))
        return copies

    far = range(n_q - 1, 1, -2)
    heard = (1,) + tuple(k - 1 for k in far)

    def send_relay(layer, i, k):
        return send(partner(1) * 2 + y, d, prod_s.at[layer, i, partner(k)],
                    relay_r.at[layer, i, k // 2], relay_sem, (layer, i, k // 2))

    def send_product(layer, i, k, source):
        to = partner(k)
        return send(to * 2 + y, d, source, prod_r.at[layer, i, q],
                    prod_sem, (layer, i, k))

    def send_last(i, cross, k):
        row = twin if cross else y
        to = partner(k)
        return send(to * 2 + row, d, prod_s.at[layers - 1, i, to, row], last_r.at[i, t],
                    last_sem, (i, cross, k))

    def send_input(layer):
        return send_twin(win.at[layer, other, :], win_v.at[layer, y], weight_sem, (layer, 0))

    def send_output(layer, which):
        return send_twin((vw, gw)[which].at[layer, :, other], out_w.at[layer, which, y],
                         weight_sem, (layer, 1 + which))

    def prepare(layer):
        half = entries // 2
        diagonal = iota((groups, groups), 0) == iota((groups, groups), 1)
        step = jnp.sum(jnp.where(diagonal, step_v[layer][None, :], 0.0), axis=1, keepdims=True)
        rate = jnp.concatenate([rate_v[layer]] * 2, axis=1)
        freq = jnp.concatenate([freq_v[layer]] * 2, axis=1)
        sign = jnp.where(iota((groups, entries), 1) < half, -1.0, 1.0)
        magnitude = jnp.exp(-rate * step)
        angle = freq * step
        keep_real = magnitude * jnp.cos(angle)
        keep_imag = magnitude * jnp.sin(angle)
        minus_one = keep_real - 1.0
        denominator = rate * rate + freq * freq
        lift_real = (-minus_one * rate + keep_imag * freq) / denominator
        lift_imag = sign * (-keep_imag * rate - minus_one * freq) / denominator
        keep_imag = sign * keep_imag

        def swap(value):
            return jnp.concatenate([value[..., half:], value[..., :half]], axis=-1)

        matrix = sin_v[layer]
        lifted = lift_real[:, None, :] * matrix + lift_imag[:, None, :] * swap(matrix)
        lifted = lifted.reshape(chans, entries)
        read = rout_v[layer].reshape(chans, entries)
        mixed = lax.dot_general(lifted, read, NT, precision=HIGHEST,
                                preferred_element_type=jnp.float32)
        first, second = iota((chans, chans), 0), iota((chans, chans), 1)
        mixed = jnp.where(first // per == second // per, mixed, 0.0)
        mixed = mixed + jnp.where(first == second, skip_v[layer][None, :], 0.0)
        old = st_v[layer]
        kept = keep_real[None] * old + keep_imag[None] * swap(old)
        base = lax.dot_general(kept.reshape(rows * groups, entries), read, NT, precision=HIGHEST,
                               preferred_element_type=jnp.float32).reshape(rows, groups, chans)
        own = iota((groups, chans), 0) == iota((groups, chans), 1) // per
        keep_v[layer] = kept
        base_v[layer] = jnp.sum(jnp.where(own[None], base, 0.0), axis=1)
        lift_v[layer] = lifted
        mix_v[layer] = mixed

    loads[0].wait()
    loads[1].wait()
    pl.semaphore_wait(barrier, n_tp - 1 + 2 * (n_dp - 1))
    sent = []
    for k in hops:
        to = partner(k)
        sent.append(send(to * 2 + y, d, xg.at[0, t], xg.at[0, t], x_sem, (0, 0, k)))
        sent.append(send(to * 2 + twin, d, tok_v, xg.at[0, t], x_sem, (0, 1, k)))
    sent.append(send_twin(tok_v, xg.at[0, t], x_sem, (0, 1, 0)))
    inputs = [send_input(0)]
    outputs = [[send_output(0, 0)]]
    for load in loads[2:9]:
        load.wait()
    prepare(0)
    for load in loads[9:]:
        load.wait()
    outs = []

    for layer in range(layers):
        for copy in sent:
            copy.wait_recv()
        x = xg[layer].reshape(batch, half).astype(jnp.float32)
        gained = (x * gain_v[layer][None, :]).astype(jnp.bfloat16)
        inputs[layer].wait_recv()
        for i in range(2):
            part = jnp.dot(gained, win_v[layer, i], preferred_element_type=jnp.float32)
            part_v[layer, pl.ds(i * n_dp, n_dp)] = part.reshape(n_dp, rows, chans)
            part_s[layer, pl.ds(i * n_dp, n_dp)] = (
                part.astype(jnp.bfloat16).reshape(n_dp, rows, chans))
        sent = send_group(lambda to: part_s.at[layer, to], part_r.at[layer, e], part_sem, layer)
        square = jnp.sum(x * x, axis=1, keepdims=True)
        eye = iota((batch, batch), 0) == iota((batch, batch), 1)
        line = jnp.sum(jnp.where(eye, square, 0.0), axis=0, keepdims=True)
        sq_s[layer] = jnp.broadcast_to(line, (8, batch))
        sent += send_group(lambda to: sq_s.at[layer], sq_r.at[layer, e], sq_sem, layer)
        if layer == 0:
            outputs[0].append(send_output(0, 1))
        total = part_v[layer, e]
        for copy in sent:
            copy.wait_recv()
        for k in range(1, n_e):
            source = lax.rem(e + n_e - k, n_e)
            total += part_r[layer, source].astype(jnp.float32)
            line += sq_r[layer, source][:1]
        pick = iota((rows, batch), 1) == iota((rows, batch), 0) + d * rows
        square = jnp.sum(jnp.where(pick, line, 0.0), axis=1, keepdims=True)
        drive = total * lax.rsqrt(square / width + epsilon)
        value = base_v[layer] + jnp.dot(drive, mix_v[layer], precision=HIGHEST,
                                        preferred_element_type=jnp.float32)
        ready[layer, e] = jax.nn.gelu(value).astype(jnp.bfloat16)
        sent = send_group(lambda to: ready.at[layer, e], ready.at[layer, e], ready_sem, layer)
        mask = iota((groups, chans), 0) == iota((groups, chans), 1) // per
        spread = jnp.where(mask[None], drive[:, None, :], 0.0).reshape(rows * groups, chans)
        push = jnp.dot(spread, lift_v[layer], precision=HIGHEST, preferred_element_type=jnp.float32)
        new_v[layer] = keep_v[layer] + push.reshape(rows, groups, entries)
        out = pltpu.make_async_copy(new_v.at[layer], out_st.at[layer], out_sem.at[layer])
        out.start()
        outs.append(out)
        for copy in outputs[layer] + sent:
            copy.wait_recv()
        first = ready[layer, pl.ds(0, n_dp)].reshape(batch, chans)
        second = ready[layer, pl.ds(n_dp, n_dp)].reshape(batch, chans)
        every = jnp.concatenate([first, second], axis=1)
        sent, relays = [], []
        for i in range(2):
            product = jnp.dot(every, out_w[layer, i].reshape(2 * chans, half),
                              preferred_element_type=jnp.float32)
            prod_s[layer, i] = product.astype(jnp.bfloat16).reshape(n_q, 2, own, half)
            if layer + 1 < layers:
                relays.append([send_relay(layer, i, k) for k in far])
            else:
                sent += [send_last(i, c, k) for k in hops if k > 1 for c in (1, 0)]
        if layer + 1 < layers:
            sent += [send_product(layer, i, 1, prod_s.at[layer, i, partner(1)]) for i in range(2)]
            for i in range(2):
                for copy, k in zip(relays[i], far):
                    copy.wait_recv()
                    joined = (prod_s[layer, i, partner(k - 1)].astype(jnp.float32)
                              + relay_r[layer, i, k // 2].astype(jnp.float32))
                    relay_s[layer, i, k // 2] = joined.astype(jnp.bfloat16)
                    sent.append(send_product(layer, i, k - 1, relay_s.at[layer, i, k // 2]))
        else:
            sent += [send_last(i, c, k) for c, k in ((1, 1), (0, 1), (1, 0)) for i in range(2)]
        if layer + 1 < layers:
            inputs.append(send_input(layer + 1))
            outputs.append([send_output(layer + 1, 0), send_output(layer + 1, 1)])
            prepare(layer + 1)
        for copy in sent:
            copy.wait_recv()
        f32 = jnp.float32
        if layer + 1 < layers:
            both = []
            for i in range(2):
                total = prod_s[layer, i, q].astype(f32)
                for k in heard:
                    total += prod_r[layer, i, partner(k)].astype(f32)
                both.append(total)
            block = pl.ds(2 * q, 2)
            current = xg[layer, block].astype(f32) + both[0] * jax.nn.sigmoid(both[1])
            xg[layer + 1, block] = current.astype(jnp.bfloat16)
            sent = []
            for k in hops:
                sent.append(send(partner(k) * 2 + y, d, xg.at[layer + 1, block],
                                 xg.at[layer + 1, block], x_sem, (layer + 1, 0, k)))
            if layer + 2 == layers:
                rest = send_twin(xg.at[layer + 1, q * 2 + twin], fin_r, fin_sem, ())
        else:
            rest.wait_recv()
            same, cross = [], []
            for i in range(2):
                total = prod_s[layer, i, q, y].astype(f32)
                for k in range(1, n_q):
                    total += last_r[i, partner(k) * 2 + y].astype(f32)
                same.append(total)
                total = last_r[i, q * 2 + twin].astype(f32)
                for k in range(1, n_q):
                    total += last_r[i, partner(k) * 2 + twin].astype(f32)
                cross.append(total)
            here = xg[layer, t].astype(f32) + same[0] * jax.nn.sigmoid(same[1])
            there = fin_r[...].astype(f32) + cross[0] * jax.nn.sigmoid(cross[1])
            out_tok[:, :half] = jnp.where(y == 0, here, there).astype(jnp.bfloat16)
            out_tok[:, half:] = jnp.where(y == 0, there, here).astype(jnp.bfloat16)
    for out in outs:
        out.wait()
    for copy in pending:
        copy.wait_send()


def body(n_tp, n_dp, *args):
    tokens, states, win = args[0], args[11], args[2]
    layers, rows, groups, entries = states.shape
    local, chans = tokens.shape[1], win.shape[2]
    own, batch, half = tokens.shape[0], rows * n_dp, local // 2
    n_q, n_e = n_tp // 2, 2 * n_dp
    f32, bf16 = jnp.float32, jnp.bfloat16
    dma = pltpu.SemaphoreType.DMA
    any_spec = pl.BlockSpec(memory_space=pl.ANY)
    scratch = [
        pltpu.VMEM((own, half), bf16),
        pltpu.VMEM((layers, half), f32),
        pltpu.VMEM((layers, 2, half, chans), bf16),
        *[pltpu.VMEM(a.shape, a.dtype) for a in args[3:9]],
        pltpu.VMEM((layers, 2, 2, chans, half), bf16),
        pltpu.VMEM(states.shape, f32),
        pltpu.VMEM((layers, n_tp, own, half), bf16),
        pltpu.VMEM((layers, 8, batch), f32),
        pltpu.VMEM((layers, n_e, 8, batch), f32),
        pltpu.VMEM((layers, n_e, rows, chans), f32),
        pltpu.VMEM((layers, n_e, rows, chans), bf16),
        pltpu.VMEM((layers, n_e, rows, chans), bf16),
        pltpu.VMEM((layers, n_e, rows, chans), bf16),
        pltpu.VMEM((layers, 2, n_q, 2, own, half), bf16),
        pltpu.VMEM((layers - 1, 2, n_q, 2, own, half), bf16),
        pltpu.VMEM((2, n_tp, own, half), bf16),
        pltpu.VMEM((own, half), bf16),
        *[pltpu.VMEM((layers - 1, 2, n_q // 2, 2, own, half), bf16)] * 2,
        pltpu.VMEM(states.shape, f32),
        pltpu.VMEM((layers, rows, chans), f32),
        pltpu.VMEM((layers, chans, entries), f32),
        pltpu.VMEM((layers, chans, chans), f32),
        pltpu.VMEM(states.shape, f32),
        dma((10 + 3 * layers,)), dma((layers,)), dma((2, layers, 2, n_q)), dma((2, layers, n_e)),
        dma((2, layers, n_e)), dma((2, layers, n_e)), dma((2, layers, 2, n_q)),
        dma((2, layers, 3)), dma((2,)), dma((2, 2, 2, n_q)),
        dma((2, layers - 1, 2, n_q // 2)),
    ]
    return pl.pallas_call(
        functools.partial(kernel, n_tp, n_dp, float(local * n_dp)),
        out_shape=(jax.ShapeDtypeStruct(tokens.shape, bf16),
                   jax.ShapeDtypeStruct(states.shape, f32)),
        in_specs=[any_spec] * 12,
        out_specs=(pl.BlockSpec(memory_space=pltpu.VMEM), any_spec),
        scratch_shapes=scratch,
        compiler_params=pltpu.CompilerParams(
            collective_id=0, has_side_effects=True, vmem_limit_bytes=67043328),
    )(*args)


def solution(mesh):
    in_specs = (
        P("tp", "dp"),
        P(None, "dp"),
        P(None, "dp", "tp"),
        P(None, "tp", None),
        P(None, "tp", None),
        P(None, "tp"),
        P(None, "tp", None, None),
        P(None, "tp", None, None),
        P(None, "tp"),
        P(None, "tp", "dp"),
        P(None, "tp", "dp"),
        P(None, "dp", "tp", None),
    )
    out_specs = (P("tp", "dp"), P(None, "dp", "tp", None))
    run = functools.partial(body, mesh.shape["tp"], mesh.shape["dp"])
    return jax.shard_map(run, mesh=mesh, in_specs=in_specs, out_specs=out_specs, check_vma=False)
```
